512 devices in a mesh: kv: 64 (over z, y), tp: 8 (over x, core).
Axes of the slice: x: 4, y: 4, z: 16, core: 2. Of those that a mesh axis runs over, the one named last changes fastest.
Arguments:
- tokens: bfloat16 [16384, 2048], P('kv'), may hold values from -40 to 40
- query_weight: bfloat16 [2048, 2048], P(None, 'tp'), may hold values from -0.125 to 0.125
- key_matrix: bfloat16 [2048, 1024], P(None, 'tp'), may hold values from -0.125 to 0.125
- value_matrix: bfloat16 [2048, 1024], P(None, 'tp'), may hold values from -0.125 to 0.125
- gate_weight: bfloat16 [2, 2048, 16], replicated, may hold values from -0.125 to 0.125
- key_pool_weight: float32 [16, 8], replicated, may hold values from -1.5 to 1.5
- value_pool_weight: float32 [16, 8], replicated, may hold values from -1.5 to 1.5
- out_weight: bfloat16 [2048, 2048], P('tp'), may hold values from -0.125 to 0.125
- chosen: int32 [256, 32], P('kv'), may hold values from 0 to 255, as said below
Outputs:
- mixed: bfloat16 [16384, 2048], P(('kv', 'tp'))
- log_sums: float32 [16384, 16], P('kv', 'tp')
The draws below stay inside these ranges and needn't reach their ends.
Inputs may be any that keep to these rules, and one draw needn't show every extreme that they name: `chosen`: row i names only blocks <= i and names block i in its first column; a block may stand several times in a row and counts each time. The rows of one index of kv name, together, at most 2 distinct blocks held by any one other index, and exactly 2 of the index just before it whenever there is one.
All inputs are finite; a program needn't handle non-finite values.
Results may differ from the reference program's by a relative error of at most 0.018.
Values may be sent and summed in bfloat16 or wider, within the bound.
No kernel may reach another device: no remote copies, remote signals or barrier semaphores. Data moves between devices by JAX's collectives and lax.ppermute only.
A program may use at most 64 MiB of HBM per device.

```python
import jax
import jax.numpy as jnp
from jax import lax

MODEL_WIDTH = 2048
QUERY_HEADS = 16
KEY_HEADS = 8
HEAD_SIZE = 128
TOKENS_PER_SHARD = 256
BLOCK_LENGTH = 64
POOL_STRIDE = 16
PICKED_BLOCKS = 32
SEQUENCE_LENGTH = 16384
KEY_BLOCK_COUNT = 256
N_TP = 8


def draw_tokens(key, part):
    base = jnp.clip(jax.random.normal(key, (SEQUENCE_LENGTH, MODEL_WIDTH), jnp.float32), -5.0, 5.0)
    return base.astype(jnp.bfloat16)


def draw_chosen(key, part):
    per_dev = TOKENS_PER_SHARD // BLOCK_LENGTH
    devices = SEQUENCE_LENGTH // TOKENS_PER_SHARD
    block_total = devices * per_dev
    keys_list = jax.random.split(jax.random.fold_in(key, 17), 6)
    first_slot = jax.random.randint(keys_list[0], (devices, devices), 0, per_dev)
    second_slot = (first_slot + jax.random.randint(keys_list[1], (devices, devices), 1, per_dev)) % per_dev
    pool_table = jnp.stack([first_slot, second_slot], axis=-1)
    block_ids = jnp.arange(block_total, dtype=jnp.int32)[:, None]
    requester = block_ids // per_dev
    local_pos = block_ids % per_dev
    pick_shape = (block_total, PICKED_BLOCKS)
    draws_a = jax.random.randint(keys_list[2], pick_shape, 0, 1 << 30)
    draws_b = jax.random.randint(keys_list[3], pick_shape, 0, 1 << 30)
    draws_c = jax.random.randint(keys_list[4], pick_shape, 0, 1 << 30)
    draws_d = jax.random.randint(keys_list[5], pick_shape, 0, 1 << 30)
    floor_owner = jnp.maximum(requester, 1)
    owners = jnp.minimum(draws_a % floor_owner, draws_b % floor_owner)
    slot_pick = draws_c % 2
    remote = owners * per_dev + pool_table[requester, owners, slot_pick]
    local_pick = requester * per_dev + draws_d % (local_pos + 1)
    use_local = (requester == 0) | (draws_c // 2 % 4 == 0)
    picked_blocks = jnp.where(use_local, local_pick, remote)
    column = jnp.arange(PICKED_BLOCKS)[None, :]
    leading = (local_pos == 0) & (requester >= 1)
    before = jnp.maximum(requester - 1, 0)
    far_owner = jnp.where(requester >= devices // 2, requester - devices // 2, before)
    picked_blocks = jnp.where(leading & (column == 1), before * per_dev + pool_table[requester, before, 0], picked_blocks)
    picked_blocks = jnp.where(leading & (column == 2), before * per_dev + pool_table[requester, before, 1], picked_blocks)
    picked_blocks = jnp.where(leading & (column == 3), far_owner * per_dev + pool_table[requester, far_owner, 0], picked_blocks)
    picked_blocks = jnp.where(column == 0, block_ids, picked_blocks)
    return picked_blocks.astype(jnp.int32)


def steps_of(stream_key, extent, shards, smallest, high):
    factor_of = 1.0
    for dim, shards_of in shards:
        heights = jax.random.uniform(jax.random.fold_in(jax.random.fold_in(stream_key, 6), dim), (shards_of,), jnp.float32, smallest / len(shards), high / len(shards))
        factor_of = factor_of * jnp.repeat(jnp.exp(heights), extent[dim] // shards_of).reshape((-1,) + (1,) * (len(extent) - 1 - dim))
    return factor_of


def centred(own_key, shape, scale, most, pieces=(), kind=jnp.bfloat16):
    level = steps_of(own_key, shape, pieces, -0.22, 0.18) if pieces else 1.0
    entries = jax.random.normal(own_key, shape, jnp.float32) * scale * level
    return jnp.minimum(jnp.maximum(entries, -most), most).astype(kind)


def setup_inputs(seed: int = 0) -> dict:
    streams_of = jax.random.split(jax.random.key(seed), 10)
    return {
        "tokens": draw_tokens(jax.random.fold_in(streams_of[9], 71), 0),
        "query_weight": centred(streams_of[1], (MODEL_WIDTH, QUERY_HEADS * HEAD_SIZE), MODEL_WIDTH ** -0.5, 0.125, ((1, 8),)),
        "key_matrix": centred(streams_of[2], (MODEL_WIDTH, KEY_HEADS * HEAD_SIZE), MODEL_WIDTH ** -0.5, 0.125, ((1, 8),)),
        "value_matrix": centred(streams_of[3], (MODEL_WIDTH, KEY_HEADS * HEAD_SIZE), MODEL_WIDTH ** -0.5, 0.125, ((1, 8),)),
        "gate_weight": centred(streams_of[4], (2, MODEL_WIDTH, QUERY_HEADS), MODEL_WIDTH ** -0.5, 0.125),
        "key_pool_weight": centred(streams_of[5], (POOL_STRIDE, KEY_HEADS), 0.3, 1.5, (), jnp.float32),
        "value_pool_weight": centred(streams_of[6], (POOL_STRIDE, KEY_HEADS), 0.3, 1.5, (), jnp.float32),
        "out_weight": centred(streams_of[7], (QUERY_HEADS * HEAD_SIZE, MODEL_WIDTH), (QUERY_HEADS * HEAD_SIZE) ** -0.5, 0.125, ((0, 8),)),
        "chosen": draw_chosen(jax.random.fold_in(streams_of[9], 71), 0),
    }


THETA = 10000.0
NEGATIVE = -1e30


def apply_rotary(values_in, positions):
    half_width = values_in.shape[-1] // 2
    inverse = THETA ** (-jnp.arange(half_width, dtype=jnp.float32) / half_width)
    angles = positions.astype(jnp.float32)[:, None] * inverse[None, :]
    cosines = jnp.cos(angles)[:, None, :]
    sines = jnp.sin(angles)[:, None, :]
    front_half = values_in[..., :half_width]
    back_half = values_in[..., half_width:]
    return jnp.concatenate([front_half * cosines - back_half * sines, back_half * cosines + front_half * sines], axis=-1)


def reference(tokens, query_weight, key_matrix, value_matrix, gate_weight, key_pool_weight, value_pool_weight, out_weight, chosen):
    group_count_heads = QUERY_HEADS // KEY_HEADS
    positions = jnp.arange(SEQUENCE_LENGTH, dtype=jnp.int32)
    query_proj = jnp.dot(tokens, query_weight, preferred_element_type=jnp.float32).reshape(SEQUENCE_LENGTH, QUERY_HEADS, HEAD_SIZE)
    key_projected = jnp.dot(tokens, key_matrix, preferred_element_type=jnp.float32).reshape(SEQUENCE_LENGTH, KEY_HEADS, HEAD_SIZE)
    value_projected = jnp.dot(tokens, value_matrix, preferred_element_type=jnp.float32).reshape(SEQUENCE_LENGTH, KEY_HEADS, HEAD_SIZE)
    query_states = apply_rotary(query_proj, positions).astype(jnp.bfloat16)
    key_states = apply_rotary(key_projected, positions).astype(jnp.bfloat16)
    value_states = value_projected.astype(jnp.bfloat16)
    pooled_key_count = SEQUENCE_LENGTH // POOL_STRIDE
    block_ends = POOL_STRIDE * jnp.arange(pooled_key_count, dtype=jnp.int32) + POOL_STRIDE - 1
    compact_keys = apply_rotary(jnp.einsum("cwyi,wy->cyi", key_projected.reshape(pooled_key_count, POOL_STRIDE, KEY_HEADS, HEAD_SIZE), key_pool_weight,
                                    precision=lax.Precision.HIGHEST), block_ends).astype(jnp.bfloat16)
    compact_values = jnp.einsum("cwyi,wy->cyi", value_projected.reshape(pooled_key_count, POOL_STRIDE, KEY_HEADS, HEAD_SIZE), value_pool_weight,
                               precision=lax.Precision.HIGHEST).astype(jnp.bfloat16)
    gate_values = jax.nn.sigmoid(jnp.stack([
        jnp.dot(tokens, gate_weight[0], preferred_element_type=jnp.float32),
        jnp.dot(tokens, gate_weight[1], preferred_element_type=jnp.float32)], axis=0))
    score_scale = HEAD_SIZE ** -0.5
    pooled_keys_f = compact_keys.astype(jnp.float32)
    pooled_values_f = compact_values.astype(jnp.float32)

    def pooled_span(start_point):
        query_row_list = lax.dynamic_slice_in_dim(query_states, start_point, TOKENS_PER_SHARD, 0).reshape(TOKENS_PER_SHARD, KEY_HEADS, group_count_heads, HEAD_SIZE)
        scores = jnp.einsum("qgjd,ngd->gjqn", query_row_list.astype(jnp.float32), pooled_keys_f) * score_scale
        row_pos = start_point + jnp.arange(TOKENS_PER_SHARD, dtype=jnp.int32)
        visible = (block_ends[None, :] <= row_pos[:, None]) | (jnp.arange(pooled_key_count)[None, :] == 0)
        masked = jnp.where(visible, scores, NEGATIVE)
        peak_value = jnp.max(masked, axis=-1, keepdims=True)
        exponent = jnp.where(visible, jnp.exp(masked - peak_value), 0.0)
        weights = (exponent / jnp.sum(exponent, axis=-1, keepdims=True)).astype(jnp.bfloat16)
        span_out = jnp.einsum("gjqn,ngd->qgjd", weights.astype(jnp.float32), pooled_values_f)
        return span_out.reshape(TOKENS_PER_SHARD, QUERY_HEADS, HEAD_SIZE)

    span_starts = TOKENS_PER_SHARD * jnp.arange(SEQUENCE_LENGTH // TOKENS_PER_SHARD, dtype=jnp.int32)
    pooled_out = lax.map(pooled_span, span_starts).reshape(SEQUENCE_LENGTH, QUERY_HEADS, HEAD_SIZE)
    key_block_rows = key_states.reshape(KEY_BLOCK_COUNT, BLOCK_LENGTH, KEY_HEADS, HEAD_SIZE)
    value_block_rows = value_states.reshape(KEY_BLOCK_COUNT, BLOCK_LENGTH, KEY_HEADS, HEAD_SIZE)

    def chosen_block(packed):
        block_number, picked_blocks = packed
        query_row_list = lax.dynamic_slice_in_dim(query_states, block_number * BLOCK_LENGTH, BLOCK_LENGTH, 0).reshape(BLOCK_LENGTH, KEY_HEADS, group_count_heads, HEAD_SIZE)
        key_row_list = key_block_rows[picked_blocks].reshape(PICKED_BLOCKS * BLOCK_LENGTH, KEY_HEADS, HEAD_SIZE).astype(jnp.float32)
        value_row_list = value_block_rows[picked_blocks].reshape(PICKED_BLOCKS * BLOCK_LENGTH, KEY_HEADS, HEAD_SIZE).astype(jnp.float32)
        scores = jnp.einsum("qgjd,kgd->gjqk", query_row_list.astype(jnp.float32), key_row_list) * score_scale
        key_pos = (picked_blocks[:, None] * BLOCK_LENGTH + jnp.arange(BLOCK_LENGTH, dtype=jnp.int32)[None, :]).reshape(-1)
        query_pos = block_number * BLOCK_LENGTH + jnp.arange(BLOCK_LENGTH, dtype=jnp.int32)
        allowed = key_pos[None, :] <= query_pos[:, None]
        masked = jnp.where(allowed, scores, NEGATIVE)
        peak_value = jnp.max(masked, axis=-1, keepdims=True)
        exponent = jnp.where(allowed, jnp.exp(masked - peak_value), 0.0)
        totals = jnp.sum(exponent, axis=-1, keepdims=True)
        weights = (exponent / totals).astype(jnp.bfloat16)
        block_out = jnp.einsum("gjqk,kgd->qgjd", weights.astype(jnp.float32), value_row_list).reshape(BLOCK_LENGTH, QUERY_HEADS, HEAD_SIZE)
        block_logs = jnp.transpose((peak_value + jnp.log(totals))[..., 0], (2, 0, 1)).reshape(BLOCK_LENGTH, QUERY_HEADS)
        return block_out, block_logs

    sel_out, log_sums = lax.map(chosen_block, (jnp.arange(KEY_BLOCK_COUNT, dtype=jnp.int32), chosen))
    sel_out = sel_out.reshape(SEQUENCE_LENGTH, QUERY_HEADS, HEAD_SIZE)
    log_sums = log_sums.reshape(SEQUENCE_LENGTH, QUERY_HEADS)
    attended = (gate_values[0][:, :, None] * pooled_out + gate_values[1][:, :, None] * sel_out)
    attended = attended.astype(jnp.bfloat16).reshape(SEQUENCE_LENGTH, QUERY_HEADS * HEAD_SIZE)
    group_width = QUERY_HEADS * HEAD_SIZE // N_TP
    summed = jnp.zeros((SEQUENCE_LENGTH, MODEL_WIDTH), jnp.float32)
    for member in range(N_TP):
        partial_value = jnp.dot(attended[:, member * group_width:(member + 1) * group_width],
                          out_weight[member * group_width:(member + 1) * group_width],
                          preferred_element_type=jnp.float32).astype(jnp.bfloat16)
        partial_value = lax.optimization_barrier(partial_value)
        summed = summed + partial_value.astype(jnp.float32)
    return summed.astype(jnp.bfloat16), log_sums
```

```python
import jax
import jax.numpy as jnp
import numpy as np
from jax import lax
from jax.experimental import pallas as pl
from jax.experimental.pallas import tpu as pltpu
from jax.sharding import Mesh
from jax.sharding import PartitionSpec as P

HEAD_SIZE = 128
BLOCK = 64
POOL_STRIDE = 16
THETA = 10000.0
NEGATIVE = -1e30
FLOOR = -1e29
KV = ("z", "y")
SPAN = 256
STATS = 16
PER_STEP = 8
SCALE = HEAD_SIZE**-0.5


def rotary_tables(start, offsets):
    half = HEAD_SIZE // 2
    inverse = THETA ** (-np.arange(half, dtype=np.float64) / half)
    local = np.asarray(offsets, np.float64)[:, None] * inverse[None, :]
    cos_l = jnp.asarray(np.cos(local), jnp.float32)
    sin_l = jnp.asarray(np.sin(local), jnp.float32)
    starts = np.arange(64, dtype=np.float64)[:, None] * SPAN * inverse[None, :]
    cos_s = lax.dynamic_slice_in_dim(jnp.asarray(np.cos(starts), jnp.float32), start, 1, 0)
    sin_s = lax.dynamic_slice_in_dim(jnp.asarray(np.sin(starts), jnp.float32), start, 1, 0)
    return cos_l * cos_s - sin_l * sin_s, sin_l * cos_s + cos_l * sin_s


def rotate(value, cosines, sines):
    half = HEAD_SIZE // 2
    front, back = value[..., :half], value[..., half:]
    return jnp.concatenate([front * cosines - back * sines, back * cosines + front * sines], -1)


def chosen_kernel(meta_ref, ids_ref, q_ref, kv_ref, out_ref, acc_ref, m_ref, l_ref, lse_ref):
    z = meta_ref[0]
    y = meta_ref[1]
    row = lax.broadcasted_iota(jnp.int32, (BLOCK, HEAD_SIZE), 0)
    lane = lax.broadcasted_iota(jnp.int32, (1, HEAD_SIZE), 1)
    lane = jnp.where(lane >= BLOCK, lane - BLOCK, lane)

    for peer in range(4):
        for qb in range(4):
            acc_ref[qb] = jnp.zeros((HEAD_SIZE, HEAD_SIZE), jnp.float32)
            m_ref[qb] = jnp.full((1, HEAD_SIZE), FLOOR, jnp.float32)
            l_ref[qb] = jnp.zeros((1, HEAD_SIZE), jnp.float32)

        def group(k, carry, peer=peer):
            for qb in range(4):
                g = peer * 4 + qb
                qpos = (z * 4 + peer) * SPAN + qb * BLOCK + lane
                keys, values, bases = [], [], []
                for e in range(PER_STEP):
                    idx = ids_ref[g * 32 + k * PER_STEP + e]
                    none = idx < 0
                    safe = jnp.where(none, 0, idx)
                    at = pl.multiple_of(safe * BLOCK, BLOCK)
                    keys.append(kv_ref[pl.ds(at, BLOCK), :HEAD_SIZE])
                    values.append(kv_ref[pl.ds(at, BLOCK), HEAD_SIZE:])
                    base = ((safe // 4) * 4 + y) * SPAN + (safe % 4) * BLOCK
                    bases.append(jnp.where(none, 1 << 30, base))
                kg = jnp.concatenate(keys, 0)
                vg = jnp.concatenate(values, 0)
                q = q_ref[g * 128 : (g + 1) * 128, :]
                s = lax.dot_general(
                    kg, q, (((1,), (1,)), ((), ())), preferred_element_type=jnp.float32
                )
                slabs = []
                for e in range(PER_STEP):
                    slab = s[e * BLOCK : (e + 1) * BLOCK] * SCALE
                    seen = row <= (qpos - bases[e])
                    slabs.append(jnp.where(seen, slab, NEGATIVE))
                s = jnp.concatenate(slabs, 0)
                m_old = m_ref[qb]
                m_new = jnp.maximum(m_old, jnp.max(s, axis=0, keepdims=True))
                alpha = jnp.exp(m_old - m_new)
                p = jnp.exp(s - m_new)
                l_ref[qb] = l_ref[qb] * alpha + jnp.sum(p, axis=0, keepdims=True)
                m_ref[qb] = m_new
                pv = lax.dot_general(
                    vg,
                    p.astype(jnp.bfloat16),
                    (((0,), (0,)), ((), ())),
                    preferred_element_type=jnp.float32,
                )
                acc_ref[qb] = acc_ref[qb] * alpha + pv
            return carry

        count = meta_ref[2 + peer]
        lax.fori_loop(0, count, group, 0)
        for qb in range(4):
            total = l_ref[qb]
            some = total > 0.0
            safe_total = jnp.where(some, total, 1.0)
            normal = acc_ref[qb] / safe_total
            out = jnp.transpose(normal).astype(jnp.bfloat16)
            for half in range(2):
                for head in range(2):
                    out_ref[
                        peer * 2 + half,
                        qb * 32 : (qb + 1) * 32,
                        head * HEAD_SIZE : (head + 1) * HEAD_SIZE,
                    ] = out[head * BLOCK + half * 32 : head * BLOCK + half * 32 + 32]
            lse_ref[peer * 4 + qb : peer * 4 + qb + 1, :] = jnp.where(
                some, m_ref[qb] + jnp.log(safe_total), FLOOR
            )

    for peer in range(4):
        lse = lse_ref[peer * 4 : peer * 4 + 4, :]
        wide = jnp.concatenate(
            [
                jnp.concatenate([lse[0:1], lse[1:2]], 1),
                jnp.concatenate([lse[2:3], lse[3:4]], 1),
            ],
            0,
        )
        high = wide.astype(jnp.bfloat16).astype(jnp.float32)
        rest = wide - high
        middle = rest.astype(jnp.bfloat16).astype(jnp.float32)
        low = rest - middle
        block = jnp.concatenate(
            [high, middle, low, jnp.zeros((STATS - 6, 2 * HEAD_SIZE), jnp.float32)], 0
        ).astype(jnp.bfloat16)
        for half in range(2):
            out_ref[peer * 2 + half, 128 : 128 + STATS, :] = block


def chosen_attention(meta, ids, queries, kv_rows):
    whole = lambda shape: pl.BlockSpec(shape, lambda i, *_: (0,) * len(shape))
    return pl.pallas_call(
        chosen_kernel,
        grid_spec=pltpu.PrefetchScalarGridSpec(
            num_scalar_prefetch=2,
            grid=(1,),
            in_specs=[whole((2048, HEAD_SIZE)), whole((4096, 2 * HEAD_SIZE))],
            out_specs=whole((8, 128 + STATS, 2 * HEAD_SIZE)),
            scratch_shapes=[
                pltpu.VMEM((4, HEAD_SIZE, HEAD_SIZE), jnp.float32),
                pltpu.VMEM((4, 1, HEAD_SIZE), jnp.float32),
                pltpu.VMEM((4, 1, HEAD_SIZE), jnp.float32),
                pltpu.VMEM((16, HEAD_SIZE), jnp.float32),
            ],
        ),
        out_shape=jax.ShapeDtypeStruct((8, 128 + STATS, 2 * HEAD_SIZE), jnp.bfloat16),
        name="chosen_attention",
    )(meta, ids, queries, kv_rows)


def shards(
    tokens,
    query_weight,
    key_matrix,
    value_matrix,
    gate_weight,
    key_pool_weight,
    value_pool_weight,
    out_weight,
    chosen,
):
    z, y = lax.axis_index("z"), lax.axis_index("y")
    x, c = lax.axis_index("x"), lax.axis_index("c")
    own = z * 4 + y
    start = own * SPAN
    group = x * 2 + c
    f32, bf16 = jnp.float32, jnp.bfloat16

    cosines, sines = rotary_tables(own, np.arange(SPAN))
    key_projected = jnp.dot(tokens, key_matrix, preferred_element_type=f32)
    value_projected = jnp.dot(tokens, value_matrix, preferred_element_type=f32)
    keys = rotate(key_projected, cosines, sines).astype(bf16)
    kv_rows = jnp.concatenate([keys, value_projected.astype(bf16)], -1)
    all_kv = lax.all_gather(kv_rows, "z", axis=0, tiled=True)

    other_weight = lax.ppermute(out_weight, "c", [(0, 1), (1, 0)])

    query_proj = jnp.dot(tokens, query_weight, preferred_element_type=f32)
    query_proj = query_proj.reshape(SPAN, 2, HEAD_SIZE)
    queries = rotate(query_proj, cosines[:, None, :], sines[:, None, :]).astype(bf16)
    by_block = queries.reshape(4, BLOCK, 2, HEAD_SIZE).transpose(0, 2, 1, 3)
    picks = jnp.pad(chosen.astype(bf16).reshape(1, 128), ((0, 15), (0, 0)))
    sent = jnp.concatenate([by_block.reshape(512, HEAD_SIZE), picks], 0)
    near = lax.all_gather(sent, "y", axis=0, tiled=False)
    near_queries = near[:, :512].reshape(2048, HEAD_SIZE)
    near_chosen = near[:, 512].reshape(16, 32).astype(jnp.int32)

    mine = ((near_chosen // 4) % 4 == y).astype(jnp.int32)
    local = (near_chosen // 16) * 4 + near_chosen % 4
    before = (np.arange(32)[:, None] < np.arange(32)[None, :]).astype(np.int32)
    rank = jnp.sum(mine[:, :, None] * before[None], axis=1)
    place = (rank[:, :, None] == np.arange(32)[None, None, :]).astype(jnp.int32)
    ids = jnp.sum(mine[:, :, None] * place * (local[:, :, None] + 1), axis=1) - 1
    steps = (jnp.max(jnp.sum(mine, axis=1).reshape(4, 4), axis=1) + PER_STEP - 1) // PER_STEP
    meta = jnp.concatenate([jnp.stack([z, y]).astype(jnp.int32), steps.astype(jnp.int32)])

    key_mix = lax.dynamic_slice_in_dim(key_pool_weight, group, 1, 1)
    value_mix = lax.dynamic_slice_in_dim(value_pool_weight, group, 1, 1)
    pooled_here = SPAN // POOL_STRIDE
    pooled_k = jnp.sum(
        key_projected.reshape(pooled_here, POOL_STRIDE, HEAD_SIZE) * key_mix[None], axis=1
    )
    pooled_v = jnp.sum(
        value_projected.reshape(pooled_here, POOL_STRIDE, HEAD_SIZE) * value_mix[None], axis=1
    )
    ends = np.arange(pooled_here) * POOL_STRIDE + POOL_STRIDE - 1
    pooled_k = rotate(pooled_k, cosines[POOL_STRIDE - 1 :: POOL_STRIDE], sines[POOL_STRIDE - 1 :: POOL_STRIDE])
    pooled = jnp.concatenate([pooled_k.astype(bf16), pooled_v.astype(bf16)], -1)
    pooled = lax.all_gather(pooled, "y", axis=0, tiled=True)
    pooled = lax.all_gather(pooled, "z", axis=0, tiled=True)
    all_keys, all_values = pooled[:, :HEAD_SIZE], pooled[:, HEAD_SIZE:]

    positions = start + jnp.arange(SPAN, dtype=jnp.int32)
    pooled_total = all_keys.shape[0]
    pooled_ends = POOL_STRIDE * jnp.arange(pooled_total, dtype=jnp.int32) + POOL_STRIDE - 1
    visible = (pooled_ends[None, :] <= positions[:, None]) | (
        jnp.arange(pooled_total)[None, :] == 0
    )
    scores = jnp.einsum("qjd,nd->jqn", queries, all_keys, preferred_element_type=f32) * SCALE
    masked = jnp.where(visible, scores, NEGATIVE)
    peak = jnp.max(masked, axis=-1, keepdims=True)
    exponent = jnp.where(visible, jnp.exp(masked - peak), 0.0)
    weights = (exponent / jnp.sum(exponent, axis=-1, keepdims=True)).astype(bf16)
    pooled_out = jnp.einsum("jqn,nd->qjd", weights, all_values, preferred_element_type=f32)
    pooled_out = pooled_out.reshape(4, 2, 32, 2 * HEAD_SIZE)
    pooled_own = lax.dynamic_index_in_dim(pooled_out, c, 1, keepdims=False)
    pooled_send = lax.dynamic_index_in_dim(pooled_out, 1 - c, 1, keepdims=False)
    pooled_got = lax.ppermute(pooled_send, "c", [(0, 1), (1, 0)])

    own_tokens = lax.dynamic_index_in_dim(
        tokens.reshape(4, 2, 32, -1), c, 1, keepdims=False
    ).reshape(128, -1)
    gate_cols = lax.dynamic_slice_in_dim(gate_weight, x * 4, 4, 2)
    gates = jax.nn.sigmoid(
        jnp.einsum("td,bdh->bth", own_tokens, gate_cols, preferred_element_type=f32)
    )
    gates = gates.reshape(2, 128, 2, 2)

    partial = chosen_attention(meta, ids.reshape(-1), near_queries, all_kv)
    got = lax.all_to_all(partial, ("y", "c"), 0, 0, tiled=True)
    got = got.reshape(4, 2, 128 + STATS, 2 * HEAD_SIZE)
    stats = got[:, :, 128:134].astype(f32)
    lse = stats[:, :, 0:2] + stats[:, :, 2:4] + stats[:, :, 4:6]
    lse = lse.reshape(4, 2, 4, 2, BLOCK)
    top = jnp.max(lse, axis=0)
    parts = jnp.exp(lse - top[None])
    sums = jnp.sum(parts, axis=0)
    log_all = top + jnp.log(sums)
    log_own = lax.dynamic_index_in_dim(log_all, c, 0, keepdims=False)
    log_sums = log_own.transpose(0, 2, 1).reshape(SPAN, 2)
    share = parts / sums[None]
    share = lax.dynamic_index_in_dim(
        share.reshape(4, 2, 4, 2, 2, 32), c, 4, keepdims=False
    )
    share = share.transpose(0, 1, 2, 4, 3).reshape(4, 2, 128, 2)
    rows = got[:, :, :128].astype(f32).reshape(4, 2, 128, 2, HEAD_SIZE)
    sel_out = jnp.sum(rows * share[..., None], axis=0)

    def attended_of(which, pooled_rows):
        sel = lax.dynamic_index_in_dim(sel_out, which, 0, keepdims=False)
        gate = lax.dynamic_index_in_dim(gates, which, 2, keepdims=False)
        mix = (
            gate[0][:, :, None] * pooled_rows.reshape(128, 2, HEAD_SIZE)
            + gate[1][:, :, None] * sel
        )
        return mix.astype(bf16).reshape(128, 2 * HEAD_SIZE)

    mine_rows = attended_of(c, pooled_own)
    other_rows = attended_of(1 - c, pooled_got)
    shares = jnp.dot(mine_rows, out_weight, preferred_element_type=f32) + jnp.dot(
        other_rows, other_weight, preferred_element_type=f32
    )
    shares = shares.astype(bf16).reshape(4, 32, -1)
    pieces = lax.all_to_all(shares, "x", 0, 0, tiled=True)
    mixed = jnp.sum(pieces.astype(f32), axis=0).astype(bf16)
    return (mixed, log_sums)


def solution(mesh):
    split = Mesh(mesh.devices.reshape(16, 4, 4, 2), ("z", "y", "x", "c"))
    tp = ("x", "c")
    placed = (
        P(KV, None),
        P(None, tp),
        P(None, tp),
        P(None, tp),
        P(),
        P(),
        P(),
        P(tp, None),
        P(KV, None),
    )
    return jax.shard_map(
        shards,
        mesh=split,
        in_specs=placed,
        out_specs=(P(KV + tp, None), P(KV, tp)),
        check_vma=False,
    )
```

```python
import jax
import jax.numpy as jnp
import numpy as np
from jax import lax
from jax.experimental import pallas as pl
from jax.experimental.pallas import tpu as pltpu
from jax.sharding import Mesh
from jax.sharding import PartitionSpec as P

HEAD_SIZE = 128
BLOCK = 64
POOL_STRIDE = 16
THETA = 10000.0
NEGATIVE = -1e30
FLOOR = -1e29
KV = ("z", "y")
SPAN = 256
STATS = 16
PER_STEP = 8
POOLED = 16
RING = 16
LIST = 32
SCALE = HEAD_SIZE**-0.5


def rotary_tables(start, offsets):
    half = HEAD_SIZE // 2
    inverse = THETA ** (-np.arange(half, dtype=np.float64) / half)
    local = np.asarray(offsets, np.float64)[:, None] * inverse[None, :]
    cos_l = jnp.asarray(np.cos(local), jnp.float32)
    sin_l = jnp.asarray(np.sin(local), jnp.float32)
    starts = np.arange(64, dtype=np.float64)[:, None] * SPAN * inverse[None, :]
    cos_s = lax.dynamic_slice_in_dim(jnp.asarray(np.cos(starts), jnp.float32), start, 1, 0)
    sin_s = lax.dynamic_slice_in_dim(jnp.asarray(np.sin(starts), jnp.float32), start, 1, 0)
    return cos_l * cos_s - sin_l * sin_s, sin_l * cos_s + cos_l * sin_s


def rotate(value, cosines, sines):
    half = HEAD_SIZE // 2
    front, back = value[..., :half], value[..., half:]
    return jnp.concatenate([front * cosines - back * sines, back * cosines + front * sines], -1)


def split_three(value):
    high = value.astype(jnp.bfloat16).astype(jnp.float32)
    rest = value - high
    middle = rest.astype(jnp.bfloat16).astype(jnp.float32)
    return [high, middle, rest - middle]


def attend_kernel(meta_ref, ids_ref, bias_ref, q_ref, *refs):
    chunk_refs = refs[:RING]
    out_ref, kv_ref, pool_ref, acc_ref, m_ref, l_ref, lse_ref = refs[RING:]
    z = meta_ref[0]
    y = meta_ref[1]
    for o in range(RING):
        kv_ref[o * SPAN : (o + 1) * SPAN, :] = chunk_refs[o][:SPAN, :]
        pool_ref[o * POOLED : (o + 1) * POOLED, :] = chunk_refs[o][SPAN:, :]
    row = lax.broadcasted_iota(jnp.int32, (BLOCK, HEAD_SIZE), 0)
    lane = lax.broadcasted_iota(jnp.int32, (1, HEAD_SIZE), 1)
    lane = jnp.where(lane >= BLOCK, lane - BLOCK, lane)

    def store(peer, qb, first, normal):
        out = jnp.transpose(normal).astype(jnp.bfloat16)
        for half in range(2):
            for head in range(2):
                at = head * BLOCK + half * 32
                out_ref[
                    peer * 2 + half,
                    first + qb * 32 : first + (qb + 1) * 32,
                    head * HEAD_SIZE : (head + 1) * HEAD_SIZE,
                ] = out[at : at + 32]

    pool_row = lax.broadcasted_iota(jnp.int32, (SPAN, 1), 0)
    offset = pool_row // POOLED
    pool_at = ((z - offset) * 4 + y) * POOLED + pool_row % POOLED
    pool_end = pool_at * POOL_STRIDE + POOL_STRIDE - 1
    pool_end = jnp.where(offset > z, 1 << 30, jnp.where(pool_at == 0, 0, pool_end))
    for peer in range(4):
        for qb in range(4):
            g = peer * 4 + qb
            qpos = (z * 4 + peer) * SPAN + qb * BLOCK + lane
            s = lax.dot_general(
                pool_ref[:, :HEAD_SIZE],
                q_ref[g * 128 : (g + 1) * 128, :],
                (((1,), (1,)), ((), ())),
                preferred_element_type=jnp.float32,
            )
            s = jnp.where(pool_end <= qpos, s * SCALE, NEGATIVE)
            m = jnp.maximum(jnp.max(s, axis=0, keepdims=True), FLOOR)
            p = jnp.exp(s - m)
            total = jnp.sum(p, axis=0, keepdims=True)
            acc = lax.dot_general(
                pool_ref[:, HEAD_SIZE:],
                p.astype(jnp.bfloat16),
                (((0,), (0,)), ((), ())),
                preferred_element_type=jnp.float32,
            )
            some = total > 0.0
            total = jnp.where(some, total, 1.0)
            store(peer, qb, 128, acc / total)
            lse_ref[16 + g : 17 + g, :] = jnp.where(some, m + jnp.log(total), FLOOR)

    for peer in range(4):
        for qb in range(4):
            acc_ref[qb] = jnp.zeros((HEAD_SIZE, HEAD_SIZE), jnp.float32)
            m_ref[qb] = jnp.full((1, HEAD_SIZE), FLOOR, jnp.float32)
            l_ref[qb] = jnp.zeros((1, HEAD_SIZE), jnp.float32)

        def group(k, carry, peer=peer):
            for qb in range(4):
                g = peer * 4 + qb
                qpos = (z * 4 + peer) * SPAN + qb * BLOCK + lane
                keys, values, bases, biases = [], [], [], []
                for e in range(PER_STEP):
                    at = g * LIST + k * PER_STEP + e
                    idx = ids_ref[at]
                    none = idx < 0
                    safe = jnp.where(none, 0, idx)
                    first = pl.multiple_of(safe * BLOCK, BLOCK)
                    keys.append(kv_ref[pl.ds(first, BLOCK), :HEAD_SIZE])
                    values.append(kv_ref[pl.ds(first, BLOCK), HEAD_SIZE:])
                    base = ((z - safe // 4) * 4 + y) * SPAN + (safe % 4) * BLOCK
                    bases.append(jnp.where(none, 1 << 30, base))
                    biases.append(bias_ref[at])
                kg = jnp.concatenate(keys, 0)
                vg = jnp.concatenate(values, 0)
                s = lax.dot_general(
                    kg,
                    q_ref[g * 128 : (g + 1) * 128, :],
                    (((1,), (1,)), ((), ())),
                    preferred_element_type=jnp.float32,
                )
                slabs = []
                for e in range(PER_STEP):
                    slab = s[e * BLOCK : (e + 1) * BLOCK] * SCALE + biases[e]
                    seen = row <= (qpos - bases[e])
                    slabs.append(jnp.where(seen, slab, NEGATIVE))
                s = jnp.concatenate(slabs, 0)
                m_old = m_ref[qb]
                m_new = jnp.maximum(m_old, jnp.max(s, axis=0, keepdims=True))
                alpha = jnp.exp(m_old - m_new)
                p = jnp.exp(s - m_new)
                l_ref[qb] = l_ref[qb] * alpha + jnp.sum(p, axis=0, keepdims=True)
                m_ref[qb] = m_new
                pv = lax.dot_general(
                    vg,
                    p.astype(jnp.bfloat16),
                    (((0,), (0,)), ((), ())),
                    preferred_element_type=jnp.float32,
                )
                acc_ref[qb] = acc_ref[qb] * alpha + pv
            return carry

        lax.fori_loop(0, meta_ref[2 + peer], group, 0)
        for qb in range(4):
            total = l_ref[qb]
            some = total > 0.0
            total = jnp.where(some, total, 1.0)
            store(peer, qb, 0, acc_ref[qb] / total)
            g = peer * 4 + qb
            lse_ref[g : g + 1, :] = jnp.where(some, m_ref[qb] + jnp.log(total), FLOOR)

    for peer in range(4):
        rows = []
        for branch in range(2):
            at = branch * 16 + peer * 4
            lse = lse_ref[at : at + 4, :]
            wide = jnp.concatenate(
                [
                    jnp.concatenate([lse[0:1], lse[1:2]], 1),
                    jnp.concatenate([lse[2:3], lse[3:4]], 1),
                ],
                0,
            )
            rows += split_three(wide)
        rows.append(jnp.zeros((STATS - 12, 2 * HEAD_SIZE), jnp.float32))
        block = jnp.concatenate(rows, 0).astype(jnp.bfloat16)
        for half in range(2):
            out_ref[peer * 2 + half, SPAN : SPAN + STATS, :] = block


def attend(meta, ids, bias, queries, chunks):
    whole = lambda shape: pl.BlockSpec(shape, lambda i, *_: (0,) * len(shape))
    return pl.pallas_call(
        attend_kernel,
        grid_spec=pltpu.PrefetchScalarGridSpec(
            num_scalar_prefetch=3,
            grid=(1,),
            in_specs=[whole((2048, HEAD_SIZE))]
            + [whole((SPAN + POOLED, 2 * HEAD_SIZE))] * RING,
            out_specs=whole((8, SPAN + STATS, 2 * HEAD_SIZE)),
            scratch_shapes=[
                pltpu.VMEM((RING * SPAN, 2 * HEAD_SIZE), jnp.bfloat16),
                pltpu.VMEM((RING * POOLED, 2 * HEAD_SIZE), jnp.bfloat16),
                pltpu.VMEM((4, HEAD_SIZE, HEAD_SIZE), jnp.float32),
                pltpu.VMEM((4, 1, HEAD_SIZE), jnp.float32),
                pltpu.VMEM((4, 1, HEAD_SIZE), jnp.float32),
                pltpu.VMEM((32, HEAD_SIZE), jnp.float32),
            ],
        ),
        out_shape=jax.ShapeDtypeStruct((8, SPAN + STATS, 2 * HEAD_SIZE), jnp.bfloat16),
        name="attend",
    )(meta, ids, bias, queries, *chunks)


def merge_kernel(meta_ref, got_ref, gate_ref, own_ref, other_ref, out_ref, log_ref, t_ref, att_ref):
    c = meta_ref[0]
    for branch in range(2):
        pieces = []
        for core in range(2):
            lses = []
            for peer in range(4):
                block = got_ref[peer * 2 + core, SPAN : SPAN + STATS, :].astype(jnp.float32)
                at = branch * 6
                lses.append(block[at : at + 2] + block[at + 2 : at + 4] + block[at + 4 : at + 6])
            top = jnp.maximum(jnp.maximum(lses[0], lses[1]), jnp.maximum(lses[2], lses[3]))
            parts = [jnp.exp(v - top) for v in lses]
            total = (parts[0] + parts[1]) + (parts[2] + parts[3])
            if branch == 0:
                log_ref[core] = top + jnp.log(total)
            for v in parts:
                share = v / total
                pieces.append(share[:, :HEAD_SIZE])
                pieces.append(share[:, HEAD_SIZE:])
        t_ref[branch] = jnp.transpose(jnp.concatenate(pieces, 0))
    for core in range(2):
        for qb in range(4):
            for head in range(2):
                cols = slice(head * HEAD_SIZE, (head + 1) * HEAD_SIZE)
                total = jnp.zeros((32, HEAD_SIZE), jnp.float32)
                for branch in range(2):
                    share = t_ref[branch, pl.ds(head * BLOCK + c * 32, 32), :]
                    part = jnp.zeros((32, HEAD_SIZE), jnp.float32)
                    for peer in range(4):
                        col = (core * 4 + peer) * 4 + (qb % 2) * 2 + qb // 2
                        first = branch * 128 + qb * 32
                        value = got_ref[peer * 2 + core, first : first + 32, cols]
                        part = part + value.astype(jnp.float32) * share[:, col : col + 1]
                    g = (1 - branch) * 4 + core * 2 + head
                    total = total + part * gate_ref[qb * 32 : (qb + 1) * 32, g : g + 1]
                att_ref[core, qb * 32 : (qb + 1) * 32, cols] = total.astype(jnp.bfloat16)
    shares = jnp.dot(att_ref[c], own_ref[...], preferred_element_type=jnp.float32)
    shares = shares + jnp.dot(att_ref[1 - c], other_ref[...], preferred_element_type=jnp.float32)
    out_ref[...] = shares.astype(jnp.bfloat16)


def merge(meta, got, gates, own_weight, other_weight):
    whole = lambda shape: pl.BlockSpec(shape, lambda i, *_: (0,) * len(shape))
    width = own_weight.shape[1]
    return pl.pallas_call(
        merge_kernel,
        grid_spec=pltpu.PrefetchScalarGridSpec(
            num_scalar_prefetch=1,
            grid=(1,),
            in_specs=[
                whole((8, SPAN + STATS, 2 * HEAD_SIZE)),
                whole((128, 8)),
                whole((2 * HEAD_SIZE, width)),
                whole((2 * HEAD_SIZE, width)),
            ],
            out_specs=[whole((128, width)), whole((2, 2, 2 * HEAD_SIZE))],
            scratch_shapes=[
                pltpu.VMEM((2, HEAD_SIZE, 32), jnp.float32),
                pltpu.VMEM((2, 128, 2 * HEAD_SIZE), jnp.bfloat16),
            ],
        ),
        out_shape=[
            jax.ShapeDtypeStruct((128, width), jnp.bfloat16),
            jax.ShapeDtypeStruct((2, 2, 2 * HEAD_SIZE), jnp.float32),
        ],
        name="merge",
    )(meta, got, gates, own_weight, other_weight)


def shards(
    tokens,
    query_weight,
    key_matrix,
    value_matrix,
    gate_weight,
    key_pool_weight,
    value_pool_weight,
    out_weight,
    chosen,
):
    z, y = lax.axis_index("z"), lax.axis_index("y")
    x, c = lax.axis_index("x"), lax.axis_index("c")
    own = z * 4 + y
    group = x * 2 + c
    f32, bf16 = jnp.float32, jnp.bfloat16

    cosines, sines = rotary_tables(own, np.arange(SPAN))
    key_projected = jnp.dot(tokens, key_matrix, preferred_element_type=f32)
    value_projected = jnp.dot(tokens, value_matrix, preferred_element_type=f32)
    keys = rotate(key_projected, cosines, sines).astype(bf16)
    key_mix = lax.dynamic_slice_in_dim(key_pool_weight, group, 1, 1)
    value_mix = lax.dynamic_slice_in_dim(value_pool_weight, group, 1, 1)
    pooled_k = jnp.sum(key_projected.reshape(POOLED, POOL_STRIDE, HEAD_SIZE) * key_mix[None], axis=1)
    pooled_v = jnp.sum(
        value_projected.reshape(POOLED, POOL_STRIDE, HEAD_SIZE) * value_mix[None], axis=1
    )
    last = slice(POOL_STRIDE - 1, None, POOL_STRIDE)
    pooled_k = rotate(pooled_k, cosines[last], sines[last])
    chunk = jnp.concatenate(
        [
            jnp.concatenate([keys, value_projected.astype(bf16)], -1),
            jnp.concatenate([pooled_k.astype(bf16), pooled_v.astype(bf16)], -1),
        ],
        0,
    )
    ring_up = [(i, (i + 1) % RING) for i in range(RING)]
    ring_down = [(i, (i - 1) % RING) for i in range(RING)]
    chunks = [None] * RING
    chunks[0] = chunk
    up = down = chunk
    for k in range(1, RING // 2 + 1):
        up = lax.ppermute(up, "z", ring_up)
        chunks[k] = up
        if k < RING // 2:
            down = lax.ppermute(down, "z", ring_down)
            chunks[RING - k] = down

    other_weight = lax.ppermute(out_weight, "c", [(0, 1), (1, 0)])

    query_proj = jnp.dot(tokens, query_weight, preferred_element_type=f32)
    query_proj = query_proj.reshape(SPAN, 2, HEAD_SIZE)
    queries = rotate(query_proj, cosines[:, None, :], sines[:, None, :]).astype(bf16)
    by_block = queries.reshape(4, BLOCK, 2, HEAD_SIZE).transpose(0, 2, 1, 3)
    picks = jnp.pad(chosen.astype(bf16).reshape(1, 128), ((0, 15), (0, 0)))
    sent = jnp.concatenate([by_block.reshape(512, HEAD_SIZE), picks], 0)
    near = lax.all_gather(sent, "y", axis=0, tiled=False)
    near_queries = near[:, :512].reshape(2048, HEAD_SIZE)
    near_chosen = near[:, 512].reshape(16, 32).astype(jnp.int32)

    mine = (near_chosen // 4) % 4 == y
    slot = ((z - near_chosen // 16) % RING) * 4 + near_chosen % 4
    slot = jnp.where(mine, slot, -1)
    counts = jnp.sum((slot[:, :, None] == np.arange(BLOCK)[None, None, :]).astype(jnp.int32), axis=1)
    present = counts > 0
    earlier = (np.arange(BLOCK)[:, None] < np.arange(BLOCK)[None, :]).astype(np.float32)
    rank = jnp.dot(present.astype(f32), earlier).astype(jnp.int32)
    hit = present[:, :, None] & (rank[:, :, None] == np.arange(LIST)[None, None, :])
    ids = jnp.sum(jnp.where(hit, np.arange(1, BLOCK + 1)[None, :, None], 0), axis=1) - 1
    times = jnp.sum(jnp.where(hit, counts[:, :, None], 0), axis=1)
    bias = jnp.log(jnp.maximum(times, 1).astype(f32))
    lengths = jnp.sum(present.astype(jnp.int32), axis=1)
    steps = (jnp.max(lengths.reshape(4, 4), axis=1) + PER_STEP - 1) // PER_STEP
    meta = jnp.concatenate([jnp.stack([z, y]).astype(jnp.int32), steps.astype(jnp.int32)])

    own_tokens = lax.dynamic_index_in_dim(
        tokens.reshape(4, 2, 32, -1), c, 1, keepdims=False
    ).reshape(128, -1)
    gate_cols = lax.dynamic_slice_in_dim(gate_weight, x * 4, 4, 2)
    gates = jax.nn.sigmoid(
        jnp.einsum("td,bdh->tbh", own_tokens, gate_cols, preferred_element_type=f32)
    ).reshape(128, 8)

    partial = attend(meta, ids.reshape(-1), bias.reshape(-1), near_queries, chunks)
    got = lax.all_to_all(partial, ("y", "c"), 0, 0, tiled=True)
    shares, log_all = merge(
        c.astype(jnp.int32).reshape(1), got, gates, out_weight, other_weight
    )
    log_own = lax.dynamic_index_in_dim(log_all, c, 0, keepdims=False)
    log_sums = log_own.reshape(4, 2, BLOCK).transpose(0, 2, 1).reshape(SPAN, 2)
    pieces = lax.all_to_all(shares.reshape(4, 32, -1), "x", 0, 0, tiled=True)
    mixed = jnp.sum(pieces.astype(f32), axis=0).astype(bf16)
    return (mixed, log_sums)


def solution(mesh):
    split = Mesh(mesh.devices.reshape(16, 4, 4, 2), ("z", "y", "x", "c"))
    tp = ("x", "c")
    placed = (
        P(KV, None),
        P(None, tp),
        P(None, tp),
        P(None, tp),
        P(),
        P(),
        P(),
        P(tp, None),
        P(KV, None),
    )
    return jax.shard_map(
        shards,
        mesh=split,
        in_specs=placed,
        out_specs=(P(KV + tp, None), P(KV, tp)),
        check_vma=False,
    )
```

```python
import jax
import jax.numpy as jnp
import numpy as np
from jax import lax
from jax.experimental import pallas as pl
from jax.experimental.pallas import tpu as pltpu
from jax.sharding import Mesh
from jax.sharding import PartitionSpec as P


HEAD_SIZE = 128
BLOCK = 64
POOL_STRIDE = 16
THETA = 10000.0
NEGATIVE = -1e30
FLOOR = -1e29
KV = ("z", "y")
SPAN = 256
STATS = 16
PER_STEP = 4
POOLED = 16
RING = 16
LIST = 32
SCALE = HEAD_SIZE**-0.5


def rotary_tables(start, offsets):
    half = HEAD_SIZE // 2
    inverse = THETA ** (-np.arange(half, dtype=np.float64) / half)
    local = np.asarray(offsets, np.float64)[:, None] * inverse[None, :]
    cos_l = jnp.asarray(np.cos(local), jnp.float32)
    sin_l = jnp.asarray(np.sin(local), jnp.float32)
    starts = np.arange(64, dtype=np.float64)[:, None] * SPAN * inverse[None, :]
    cos_s = lax.dynamic_slice_in_dim(jnp.asarray(np.cos(starts), jnp.float32), start, 1, 0)
    sin_s = lax.dynamic_slice_in_dim(jnp.asarray(np.sin(starts), jnp.float32), start, 1, 0)
    return cos_l * cos_s - sin_l * sin_s, sin_l * cos_s + cos_l * sin_s


def rotate(value, cosines, sines):
    half = HEAD_SIZE // 2
    front, back = value[..., :half], value[..., half:]
    return jnp.concatenate([front * cosines - back * sines, back * cosines + front * sines], -1)


def project_kernel(
    meta_ref, tok_ref, wk_ref, wv_ref, kmix_ref, vmix_ref, local_ref, span_ref, out_ref, k_ref, v_ref
):
    step = pl.program_id(0)

    @pl.when(step == 0)
    def _():
        k_ref[...] = jnp.zeros_like(k_ref)
        v_ref[...] = jnp.zeros_like(v_ref)

    k_ref[...] += jnp.dot(tok_ref[...], wk_ref[...], preferred_element_type=jnp.float32)
    v_ref[...] += jnp.dot(tok_ref[...], wv_ref[...], preferred_element_type=jnp.float32)

    @pl.when(step == pl.num_programs(0) - 1)
    def _():
        own = meta_ref[0]
        group = meta_ref[1]
        cos_s = span_ref[0, pl.ds(own, 1), :]
        sin_s = span_ref[1, pl.ds(own, 1), :]

        def rotated(value, cos_l, sin_l):
            cosines = cos_l * cos_s - sin_l * sin_s
            sines = sin_l * cos_s + cos_l * sin_s
            sign = lax.broadcasted_iota(jnp.int32, (1, HEAD_SIZE), 1) < HEAD_SIZE // 2
            turned = pltpu.roll(value, HEAD_SIZE // 2, 1)
            return value * cosines + jnp.where(sign, -turned, turned) * sines

        def pooled(value, mix_ref):
            lane = lax.broadcasted_iota(jnp.int32, (POOL_STRIDE, 8), 1)
            mix = jnp.sum(jnp.where(lane == group, mix_ref[...], 0.0), axis=1, keepdims=True)
            mixed = value.reshape(POOLED, POOL_STRIDE, HEAD_SIZE) * mix[None]
            return jnp.sum(mixed, axis=1)

        keys = k_ref[...]
        values = v_ref[...]
        out_ref[:SPAN, :HEAD_SIZE] = rotated(
            keys, local_ref[0, :SPAN], local_ref[1, :SPAN]
        ).astype(jnp.bfloat16)
        out_ref[:SPAN, HEAD_SIZE:] = values.astype(jnp.bfloat16)
        out_ref[SPAN:, :HEAD_SIZE] = rotated(
            pooled(keys, kmix_ref), local_ref[0, SPAN:], local_ref[1, SPAN:]
        ).astype(jnp.bfloat16)
        out_ref[SPAN:, HEAD_SIZE:] = pooled(values, vmix_ref).astype(jnp.bfloat16)


def project(meta, tokens, key_matrix, value_matrix, key_mix, value_mix):
    half = HEAD_SIZE // 2
    inverse = THETA ** (-np.arange(half, dtype=np.float64) / half)
    inverse = np.concatenate([inverse, inverse])
    offsets = np.concatenate(
        [np.arange(SPAN), np.arange(POOLED) * POOL_STRIDE + POOL_STRIDE - 1]
    ).astype(np.float64)
    local = offsets[:, None] * inverse[None, :]
    spans = np.arange(64, dtype=np.float64)[:, None] * SPAN * inverse[None, :]
    local = jnp.asarray(np.stack([np.cos(local), np.sin(local)]), jnp.float32)
    spans = jnp.asarray(np.stack([np.cos(spans), np.sin(spans)]), jnp.float32)
    depth = 512
    return pl.pallas_call(
        project_kernel,
        grid_spec=pltpu.PrefetchScalarGridSpec(
            num_scalar_prefetch=1,
            grid=(tokens.shape[1] // depth,),
            in_specs=[
                pl.BlockSpec((SPAN, depth), lambda i, *_: (0, i)),
                pl.BlockSpec((depth, HEAD_SIZE), lambda i, *_: (i, 0)),
                pl.BlockSpec((depth, HEAD_SIZE), lambda i, *_: (i, 0)),
                pl.BlockSpec((POOL_STRIDE, 8), lambda i, *_: (0, 0)),
                pl.BlockSpec((POOL_STRIDE, 8), lambda i, *_: (0, 0)),
                pl.BlockSpec((2, SPAN + POOLED, HEAD_SIZE), lambda i, *_: (0, 0, 0)),
                pl.BlockSpec((2, 64, HEAD_SIZE), lambda i, *_: (0, 0, 0)),
            ],
            out_specs=pl.BlockSpec((SPAN + POOLED, 2 * HEAD_SIZE), lambda i, *_: (0, 0)),
            scratch_shapes=[
                pltpu.VMEM((SPAN, HEAD_SIZE), jnp.float32),
                pltpu.VMEM((SPAN, HEAD_SIZE), jnp.float32),
            ],
        ),
        out_shape=jax.ShapeDtypeStruct((SPAN + POOLED, 2 * HEAD_SIZE), jnp.bfloat16),
        compiler_params=pltpu.CompilerParams(vmem_limit_bytes=12 << 20),
        name="project",
    )(meta, tokens, key_matrix, value_matrix, key_mix, value_mix, local, spans)


def split_three(value):
    high = value.astype(jnp.bfloat16).astype(jnp.float32)
    rest = value - high
    middle = rest.astype(jnp.bfloat16).astype(jnp.float32)
    return [high, middle, rest - middle]


def attend_kernel(meta_ref, ids_ref, bias_ref, *refs):
    q_refs = refs[:4]
    chunk_refs = refs[4 : 4 + RING]
    out_ref, kv_ref, pool_ref, acc_ref, m_ref, l_ref, lse_ref = refs[4 + RING :]
    z = meta_ref[0]
    y = meta_ref[1]
    owners = [(y + peer) % 4 for peer in range(4)]
    for o in range(RING):
        kv_ref[o * SPAN : (o + 1) * SPAN, :] = chunk_refs[o][:SPAN, :]
        pool_ref[o * POOLED : (o + 1) * POOLED, :] = chunk_refs[o][SPAN:, :]
    row = lax.broadcasted_iota(jnp.int32, (BLOCK, HEAD_SIZE), 0)
    lane = lax.broadcasted_iota(jnp.int32, (1, HEAD_SIZE), 1)
    lane = jnp.where(lane >= BLOCK, lane - BLOCK, lane)

    def store(peer, qb, first, normal):
        out = jnp.transpose(normal).astype(jnp.bfloat16)
        for half in range(2):
            for head in range(2):
                at = head * BLOCK + half * 32
                out_ref[
                    owners[peer] * 2 + half,
                    first + qb * 32 : first + (qb + 1) * 32,
                    head * HEAD_SIZE : (head + 1) * HEAD_SIZE,
                ] = out[at : at + 32]

    col = lax.broadcasted_iota(jnp.int32, (1, RING * POOLED), 1)
    offset = col // POOLED
    pool_at = ((z - offset) * 4 + y) * POOLED + col % POOLED
    pool_end = pool_at * POOL_STRIDE + POOL_STRIDE - 1
    pool_end = jnp.where(offset > z, 1 << 30, jnp.where(pool_at == 0, 0, pool_end))
    q_row = lax.broadcasted_iota(jnp.int32, (512, 1), 0)
    q_row = (q_row // 128) * BLOCK + q_row % BLOCK
    eye = lax.broadcasted_iota(jnp.int32, (128, 128), 0) == lax.broadcasted_iota(
        jnp.int32, (128, 128), 1
    )
    for peer in range(4):
        s = lax.dot_general(
            q_refs[peer][:512, :],
            pool_ref[:, :HEAD_SIZE],
            (((1,), (1,)), ((), ())),
            preferred_element_type=jnp.float32,
        )
        s = jnp.where(pool_end <= (z * 4 + owners[peer]) * SPAN + q_row, s * SCALE, NEGATIVE)
        m = jnp.maximum(jnp.max(s, axis=1, keepdims=True), FLOOR)
        p = jnp.exp(s - m)
        total = jnp.sum(p, axis=1, keepdims=True)
        acc = jnp.dot(
            p.astype(jnp.bfloat16), pool_ref[:, HEAD_SIZE:], preferred_element_type=jnp.float32
        )
        some = total > 0.0
        total = jnp.where(some, total, 1.0)
        lse = jnp.where(some, m + jnp.log(total), FLOOR)
        out = (acc / total).astype(jnp.bfloat16)
        for qb in range(4):
            for head in range(2):
                for half in range(2):
                    at = qb * 128 + head * BLOCK + half * 32
                    out_ref[
                        owners[peer] * 2 + half,
                        128 + qb * 32 : 128 + (qb + 1) * 32,
                        head * HEAD_SIZE : (head + 1) * HEAD_SIZE,
                    ] = out[at : at + 32]
            spread = jnp.where(eye, lse[qb * 128 : (qb + 1) * 128], 0.0)
            g = 16 + peer * 4 + qb
            lse_ref[g : g + 1, :] = jnp.sum(spread, axis=0, keepdims=True)

    for peer in range(4):
        for qb in range(4):
            acc_ref[qb] = jnp.zeros((HEAD_SIZE, HEAD_SIZE), jnp.float32)
            m_ref[qb] = jnp.full((1, HEAD_SIZE), FLOOR, jnp.float32)
            l_ref[qb] = jnp.zeros((1, HEAD_SIZE), jnp.float32)

        def group(k, carry, peer=peer):
            for qb in range(4):
                g = peer * 4 + qb
                qpos = (z * 4 + owners[peer]) * SPAN + qb * BLOCK + lane
                keys, values, bases, biases = [], [], [], []
                for e in range(PER_STEP):
                    idx = ids_ref[g, k * PER_STEP + e]
                    none = idx < 0
                    safe = jnp.where(none, 0, idx)
                    first = pl.multiple_of(safe * BLOCK, BLOCK)
                    keys.append(kv_ref[pl.ds(first, BLOCK), :HEAD_SIZE])
                    values.append(kv_ref[pl.ds(first, BLOCK), HEAD_SIZE:])
                    base = ((z - safe // 4) * 4 + y) * SPAN + (safe % 4) * BLOCK
                    bases.append(jnp.where(none, 1 << 30, base))
                    biases.append(bias_ref[g, k * PER_STEP + e])
                kg = jnp.concatenate(keys, 0)
                vg = jnp.concatenate(values, 0)
                s = lax.dot_general(
                    kg,
                    q_refs[peer][qb * 128 : (qb + 1) * 128, :],
                    (((1,), (1,)), ((), ())),
                    preferred_element_type=jnp.float32,
                )
                slabs = []
                for e in range(PER_STEP):
                    slab = s[e * BLOCK : (e + 1) * BLOCK] * SCALE + biases[e]
                    seen = row <= (qpos - bases[e])
                    slabs.append(jnp.where(seen, slab, NEGATIVE))
                s = jnp.concatenate(slabs, 0)
                m_old = m_ref[qb]
                m_new = jnp.maximum(m_old, jnp.max(s, axis=0, keepdims=True))
                alpha = jnp.exp(m_old - m_new)
                p = jnp.exp(s - m_new)
                l_ref[qb] = l_ref[qb] * alpha + jnp.sum(p, axis=0, keepdims=True)
                m_ref[qb] = m_new
                pv = lax.dot_general(
                    vg,
                    p.astype(jnp.bfloat16),
                    (((0,), (0,)), ((), ())),
                    preferred_element_type=jnp.float32,
                )
                acc_ref[qb] = acc_ref[qb] * alpha + pv
            return carry

        lax.fori_loop(0, meta_ref[2 + peer], group, 0)
        for qb in range(4):
            total = l_ref[qb]
            some = total > 0.0
            total = jnp.where(some, total, 1.0)
            store(peer, qb, 0, acc_ref[qb] / total)
            g = peer * 4 + qb
            lse_ref[g : g + 1, :] = jnp.where(some, m_ref[qb] + jnp.log(total), FLOOR)

    for peer in range(4):
        rows = []
        for branch in range(2):
            at = branch * 16 + peer * 4
            lse = lse_ref[at : at + 4, :]
            wide = jnp.concatenate(
                [
                    jnp.concatenate([lse[0:1], lse[1:2]], 1),
                    jnp.concatenate([lse[2:3], lse[3:4]], 1),
                ],
                0,
            )
            rows += split_three(wide)
        rows.append(jnp.zeros((STATS - 12, 2 * HEAD_SIZE), jnp.float32))
        block = jnp.concatenate(rows, 0).astype(jnp.bfloat16)
        for half in range(2):
            out_ref[owners[peer] * 2 + half, SPAN : SPAN + STATS, :] = block


def attend(meta, ids, bias, queries, chunks):
    whole = lambda shape: pl.BlockSpec(shape, lambda i, *_: (0,) * len(shape))
    return pl.pallas_call(
        attend_kernel,
        grid_spec=pltpu.PrefetchScalarGridSpec(
            num_scalar_prefetch=3,
            grid=(1,),
            in_specs=[whole((528, HEAD_SIZE))] * 4
            + [whole((SPAN + POOLED, 2 * HEAD_SIZE))] * RING,
            out_specs=whole((8, SPAN + STATS, 2 * HEAD_SIZE)),
            scratch_shapes=[
                pltpu.VMEM((RING * SPAN, 2 * HEAD_SIZE), jnp.bfloat16),
                pltpu.VMEM((RING * POOLED, 2 * HEAD_SIZE), jnp.bfloat16),
                pltpu.VMEM((4, HEAD_SIZE, HEAD_SIZE), jnp.float32),
                pltpu.VMEM((4, 1, HEAD_SIZE), jnp.float32),
                pltpu.VMEM((4, 1, HEAD_SIZE), jnp.float32),
                pltpu.VMEM((32, HEAD_SIZE), jnp.float32),
            ],
        ),
        out_shape=jax.ShapeDtypeStruct((8, SPAN + STATS, 2 * HEAD_SIZE), jnp.bfloat16),
        compiler_params=pltpu.CompilerParams(vmem_limit_bytes=20 << 20),
        name="attend",
    )(meta, ids, bias, *queries, *chunks)


def merge_kernel(meta_ref, got_ref, gate_ref, own_ref, other_ref, out_ref, log_ref, t_ref, att_ref):
    c = meta_ref[0]
    for branch in range(2):
        pieces = []
        for core in range(2):
            lses = []
            for peer in range(4):
                block = got_ref[peer * 2 + core, SPAN : SPAN + STATS, :].astype(jnp.float32)
                at = branch * 6
                lses.append(block[at : at + 2] + block[at + 2 : at + 4] + block[at + 4 : at + 6])
            top = jnp.maximum(jnp.maximum(lses[0], lses[1]), jnp.maximum(lses[2], lses[3]))
            parts = [jnp.exp(v - top) for v in lses]
            total = (parts[0] + parts[1]) + (parts[2] + parts[3])
            if branch == 0:
                log_ref[core] = top + jnp.log(total)
            for v in parts:
                share = v / total
                pieces.append(share[:, :HEAD_SIZE])
                pieces.append(share[:, HEAD_SIZE:])
        t_ref[branch] = jnp.transpose(jnp.concatenate(pieces, 0))
    for core in range(2):
        for qb in range(4):
            for head in range(2):
                cols = slice(head * HEAD_SIZE, (head + 1) * HEAD_SIZE)
                total = jnp.zeros((32, HEAD_SIZE), jnp.float32)
                for branch in range(2):
                    share = t_ref[branch, pl.ds(head * BLOCK + c * 32, 32), :]
                    part = jnp.zeros((32, HEAD_SIZE), jnp.float32)
                    for peer in range(4):
                        col = (core * 4 + peer) * 4 + (qb % 2) * 2 + qb // 2
                        first = branch * 128 + qb * 32
                        value = got_ref[peer * 2 + core, first : first + 32, cols]
                        part = part + value.astype(jnp.float32) * share[:, col : col + 1]
                    g = (1 - branch) * 4 + core * 2 + head
                    total = total + part * gate_ref[qb * 32 : (qb + 1) * 32, g : g + 1]
                att_ref[core, qb * 32 : (qb + 1) * 32, cols] = total.astype(jnp.bfloat16)
    shares = jnp.dot(att_ref[c], own_ref[...], preferred_element_type=jnp.float32)
    shares = shares + jnp.dot(att_ref[1 - c], other_ref[...], preferred_element_type=jnp.float32)
    out_ref[...] = shares.astype(jnp.bfloat16)


def merge(meta, got, gates, own_weight, other_weight):
    whole = lambda shape: pl.BlockSpec(shape, lambda i, *_: (0,) * len(shape))
    width = own_weight.shape[1]
    return pl.pallas_call(
        merge_kernel,
        grid_spec=pltpu.PrefetchScalarGridSpec(
            num_scalar_prefetch=1,
            grid=(1,),
            in_specs=[
                whole((8, SPAN + STATS, 2 * HEAD_SIZE)),
                whole((128, 8)),
                whole((2 * HEAD_SIZE, width)),
                whole((2 * HEAD_SIZE, width)),
            ],
            out_specs=[whole((128, width)), whole((2, 2, 2 * HEAD_SIZE))],
            scratch_shapes=[
                pltpu.VMEM((2, HEAD_SIZE, 32), jnp.float32),
                pltpu.VMEM((2, 128, 2 * HEAD_SIZE), jnp.bfloat16),
            ],
        ),
        out_shape=[
            jax.ShapeDtypeStruct((128, width), jnp.bfloat16),
            jax.ShapeDtypeStruct((2, 2, 2 * HEAD_SIZE), jnp.float32),
        ],
        compiler_params=pltpu.CompilerParams(vmem_limit_bytes=12 << 20),
        name="merge",
    )(meta, got, gates, own_weight, other_weight)


def block_lists(near, z, y):
    f32 = jnp.float32
    near_chosen = jnp.stack([v[512] for v in near]).reshape(16, 32).astype(jnp.int32)
    mine = (near_chosen // 4) % 4 == y
    slot = ((z - near_chosen // 16) % RING) * 4 + near_chosen % 4
    slot = jnp.where(mine, slot, -1)
    counts = jnp.sum((slot[:, :, None] == np.arange(BLOCK)[None, None, :]).astype(jnp.int32), axis=1)
    present = counts > 0
    earlier = (np.arange(BLOCK)[:, None] < np.arange(BLOCK)[None, :]).astype(np.float32)
    rank = jnp.dot(present.astype(f32), earlier).astype(jnp.int32)
    hit = present[:, :, None] & (rank[:, :, None] == np.arange(LIST)[None, None, :])
    ids = jnp.sum(jnp.where(hit, np.arange(1, BLOCK + 1)[None, :, None], 0), axis=1) - 1
    times = jnp.sum(jnp.where(hit, counts[:, :, None], 0), axis=1)
    bias = jnp.log(jnp.maximum(times, 1).astype(f32))
    lengths = jnp.sum(present.astype(jnp.int32), axis=1)
    steps = (jnp.max(lengths.reshape(4, 4), axis=1) + PER_STEP - 1) // PER_STEP
    meta = jnp.concatenate([jnp.stack([z, y]).astype(jnp.int32), steps.astype(jnp.int32)])
    return meta, ids, bias


def shards(
    tokens,
    query_weight,
    key_matrix,
    value_matrix,
    gate_weight,
    key_pool_weight,
    value_pool_weight,
    out_weight,
    chosen,
):
    z, y = lax.axis_index("z"), lax.axis_index("y")
    x, c = lax.axis_index("x"), lax.axis_index("c")
    own = z * 4 + y
    group = x * 2 + c
    f32, bf16 = jnp.float32, jnp.bfloat16

    cosines, sines = rotary_tables(own, np.arange(SPAN))
    place = jnp.stack([own, group]).astype(jnp.int32)
    chunk = project(place, tokens, key_matrix, value_matrix, key_pool_weight, value_pool_weight)
    query_proj = jnp.dot(tokens, query_weight, preferred_element_type=f32)
    query_proj = query_proj.reshape(SPAN, 2, HEAD_SIZE)
    queries = rotate(query_proj, cosines[:, None, :], sines[:, None, :]).astype(bf16)
    by_block = queries.reshape(4, BLOCK, 2, HEAD_SIZE).transpose(0, 2, 1, 3)
    picks = jnp.pad(chosen.astype(bf16).reshape(1, 128), ((0, 15), (0, 0)))
    sent = jnp.concatenate([by_block.reshape(512, HEAD_SIZE), picks], 0)

    ring_up = [(i, (i + 1) % RING) for i in range(RING)]
    ring_down = [(i, (i - 1) % RING) for i in range(RING)]
    chunks = [None] * RING
    chunks[0] = chunk
    up = down = chunk
    near = [sent]

    for k in range(1, RING // 2 + 1):
        up = lax.ppermute(up, "z", ring_up)
        chunks[k] = up
        if k < RING // 2:
            down = lax.ppermute(down, "z", ring_down)
            chunks[RING - k] = down
        if 1 <= k <= 3:
            pairs = [(i, (i - k) % 4) for i in range(4)]
            near.append(lax.ppermute(sent, "y", pairs))
        if k == 4:
            other_weight = lax.ppermute(out_weight, "c", [(0, 1), (1, 0)])

    meta, ids, bias = block_lists(near, z, y)

    own_tokens = lax.dynamic_index_in_dim(
        tokens.reshape(4, 2, 32, -1), c, 1, keepdims=False
    ).reshape(128, -1)
    gate_cols = lax.dynamic_slice_in_dim(gate_weight, x * 4, 4, 2)
    gates = jax.nn.sigmoid(
        jnp.einsum("td,bdh->tbh", own_tokens, gate_cols, preferred_element_type=f32)
    ).reshape(128, 8)

    partial = attend(meta, ids, bias, near, chunks)
    got = lax.all_to_all(partial, ("y", "c"), 0, 0, tiled=True)
    shares, log_all = merge(
        c.astype(jnp.int32).reshape(1), got, gates, out_weight, other_weight
    )
    log_own = lax.dynamic_index_in_dim(log_all, c, 0, keepdims=False)
    log_sums = log_own.reshape(4, 2, BLOCK).transpose(0, 2, 1).reshape(SPAN, 2)
    pieces = lax.all_to_all(shares.reshape(4, 32, -1), "x", 0, 0, tiled=True)
    mixed = jnp.sum(pieces.astype(f32), axis=0).astype(bf16)
    return (mixed, log_sums)


def solution(mesh):
    split = Mesh(mesh.devices.reshape(16, 4, 4, 2), ("z", "y", "x", "c"))
    tp = ("x", "c")
    placed = (
        P(KV, None),
        P(None, tp),
        P(None, tp),
        P(None, tp),
        P(),
        P(),
        P(),
        P(tp, None),
        P(KV, None),
    )
    return jax.shard_map(
        shards,
        mesh=split,
        in_specs=placed,
        out_specs=(P(KV + tp, None), P(KV, tp)),
        check_vma=False,
    )
```

```python
import jax
import jax.numpy as jnp
import numpy as np
from jax import lax
from jax.experimental import pallas as pl
from jax.experimental.pallas import tpu as pltpu
from jax.sharding import Mesh
from jax.sharding import PartitionSpec as P


HEAD_SIZE = 128
BLOCK = 64
POOL_STRIDE = 16
THETA = 10000.0
NEGATIVE = -1e30
FLOOR = -1e29
KV = ("z", "y")
SPAN = 256
STATS = 16
PER_STEP = 10
PEERS = 1
POOLED = 16
RING = 16
QROWS = 528
SCALE = HEAD_SIZE**-0.5


def rotary_tables(start, offsets):
    half = HEAD_SIZE // 2
    inverse = THETA ** (-np.arange(half, dtype=np.float64) / half)
    local = np.asarray(offsets, np.float64)[:, None] * inverse[None, :]
    cos_l = jnp.asarray(np.cos(local), jnp.float32)
    sin_l = jnp.asarray(np.sin(local), jnp.float32)
    starts = np.arange(64, dtype=np.float64)[:, None] * SPAN * inverse[None, :]
    cos_s = lax.dynamic_slice_in_dim(jnp.asarray(np.cos(starts), jnp.float32), start, 1, 0)
    sin_s = lax.dynamic_slice_in_dim(jnp.asarray(np.sin(starts), jnp.float32), start, 1, 0)
    return cos_l * cos_s - sin_l * sin_s, sin_l * cos_s + cos_l * sin_s


def rotate(value, cosines, sines):
    half = HEAD_SIZE // 2
    front, back = value[..., :half], value[..., half:]
    return jnp.concatenate([front * cosines - back * sines, back * cosines + front * sines], -1)


def project_kernel(
    meta_ref, tok_ref, wk_ref, wv_ref, kmix_ref, vmix_ref, local_ref, span_ref, out_ref, k_ref, v_ref
):
    step = pl.program_id(0)

    @pl.when(step == 0)
    def _():
        k_ref[...] = jnp.zeros_like(k_ref)
        v_ref[...] = jnp.zeros_like(v_ref)

    k_ref[...] += jnp.dot(tok_ref[...], wk_ref[...], preferred_element_type=jnp.float32)
    v_ref[...] += jnp.dot(tok_ref[...], wv_ref[...], preferred_element_type=jnp.float32)

    @pl.when(step == pl.num_programs(0) - 1)
    def _():
        own = meta_ref[0]
        group = meta_ref[1]
        cos_s = span_ref[0, pl.ds(own, 1), :]
        sin_s = span_ref[1, pl.ds(own, 1), :]

        def rotated(value, cos_l, sin_l):
            cosines = cos_l * cos_s - sin_l * sin_s
            sines = sin_l * cos_s + cos_l * sin_s
            sign = lax.broadcasted_iota(jnp.int32, (1, HEAD_SIZE), 1) < HEAD_SIZE // 2
            turned = pltpu.roll(value, HEAD_SIZE // 2, 1)
            return value * cosines + jnp.where(sign, -turned, turned) * sines

        def pooled(value, mix_ref):
            shape = (POOL_STRIDE, POOL_STRIDE)
            eye = lax.broadcasted_iota(jnp.int32, shape, 0) == lax.broadcasted_iota(
                jnp.int32, shape, 1
            )
            mix = jnp.where(eye, mix_ref[pl.ds(group, 1), :], 0.0)
            mix = jnp.sum(mix, axis=1, keepdims=True)
            mixed = value.reshape(POOLED, POOL_STRIDE, HEAD_SIZE) * mix[None]
            return jnp.sum(mixed, axis=1)

        keys = k_ref[...]
        values = v_ref[...]
        out_ref[:SPAN, :HEAD_SIZE] = rotated(
            keys, local_ref[0, :SPAN], local_ref[1, :SPAN]
        ).astype(jnp.bfloat16)
        out_ref[:SPAN, HEAD_SIZE:] = values.astype(jnp.bfloat16)
        out_ref[SPAN:, :HEAD_SIZE] = rotated(
            pooled(keys, kmix_ref), local_ref[0, SPAN:], local_ref[1, SPAN:]
        ).astype(jnp.bfloat16)
        out_ref[SPAN:, HEAD_SIZE:] = pooled(values, vmix_ref).astype(jnp.bfloat16)


def project(meta, tokens, key_matrix, value_matrix, key_mix, value_mix):
    half = HEAD_SIZE // 2
    inverse = THETA ** (-np.arange(half, dtype=np.float64) / half)
    inverse = np.concatenate([inverse, inverse])
    offsets = np.concatenate(
        [np.arange(SPAN), np.arange(POOLED) * POOL_STRIDE + POOL_STRIDE - 1]
    ).astype(np.float64)
    local = offsets[:, None] * inverse[None, :]
    spans = np.arange(64, dtype=np.float64)[:, None] * SPAN * inverse[None, :]
    local = jnp.asarray(np.stack([np.cos(local), np.sin(local)]), jnp.float32)
    spans = jnp.asarray(np.stack([np.cos(spans), np.sin(spans)]), jnp.float32)
    depth = 512
    return pl.pallas_call(
        project_kernel,
        grid_spec=pltpu.PrefetchScalarGridSpec(
            num_scalar_prefetch=1,
            grid=(tokens.shape[1] // depth,),
            in_specs=[
                pl.BlockSpec((SPAN, depth), lambda i, *_: (0, i)),
                pl.BlockSpec((depth, HEAD_SIZE), lambda i, *_: (i, 0)),
                pl.BlockSpec((depth, HEAD_SIZE), lambda i, *_: (i, 0)),
                pl.BlockSpec((8, POOL_STRIDE), lambda i, *_: (0, 0)),
                pl.BlockSpec((8, POOL_STRIDE), lambda i, *_: (0, 0)),
                pl.BlockSpec((2, SPAN + POOLED, HEAD_SIZE), lambda i, *_: (0, 0, 0)),
                pl.BlockSpec((2, 64, HEAD_SIZE), lambda i, *_: (0, 0, 0)),
            ],
            out_specs=pl.BlockSpec((SPAN + POOLED, 2 * HEAD_SIZE), lambda i, *_: (0, 0)),
            scratch_shapes=[
                pltpu.VMEM((SPAN, HEAD_SIZE), jnp.float32),
                pltpu.VMEM((SPAN, HEAD_SIZE), jnp.float32),
            ],
        ),
        out_shape=jax.ShapeDtypeStruct((SPAN + POOLED, 2 * HEAD_SIZE), jnp.bfloat16),
        name="project",
    )(meta, tokens, key_matrix, value_matrix, key_mix, value_mix, local, spans)


def split_three(value):
    high = value.astype(jnp.bfloat16).astype(jnp.float32)
    rest = value - high
    middle = rest.astype(jnp.bfloat16).astype(jnp.float32)
    return [high, middle, rest - middle]


def attend_kernel(meta_ref, ids_ref, bias_ref, *refs):
    own_ref, side_ref, far_ref = refs[:3]
    chunk_refs = refs[3 : 3 + RING]
    out_ref, kv_ref, pool_ref, acc_ref, m_ref, l_ref, lse_ref = refs[3 + RING :]
    z = meta_ref[0, 0]
    y = meta_ref[0, 1]
    q_refs = [own_ref, side_ref, far_ref.at[:QROWS], far_ref.at[QROWS:]]
    owners = [y ^ peer for peer in range(4)]
    for o in range(RING):
        kv_ref[o * SPAN : (o + 1) * SPAN, :] = chunk_refs[o][:SPAN, :]
        pool_ref[o * POOLED : (o + 1) * POOLED, :] = chunk_refs[o][SPAN:, :]
    row = lax.broadcasted_iota(jnp.int32, (BLOCK, HEAD_SIZE), 0)
    lane = lax.broadcasted_iota(jnp.int32, (1, HEAD_SIZE), 1)
    lane = jnp.where(lane >= BLOCK, lane - BLOCK, lane)

    def store(peer, qb, first, normal):
        out = jnp.transpose(normal).astype(jnp.bfloat16)
        for half in range(2):
            for head in range(2):
                at = head * BLOCK + half * 32
                out_ref[
                    owners[peer] * 2 + half,
                    first + qb * 32 : first + (qb + 1) * 32,
                    head * HEAD_SIZE : (head + 1) * HEAD_SIZE,
                ] = out[at : at + 32]

    col = lax.broadcasted_iota(jnp.int32, (1, RING * POOLED), 1)
    offset = col // POOLED
    pool_at = ((z - offset) * 4 + y) * POOLED + col % POOLED
    pool_end = pool_at * POOL_STRIDE + POOL_STRIDE - 1
    pool_end = jnp.where(offset > z, 1 << 30, jnp.where(pool_at == 0, 0, pool_end))
    q_row = lax.broadcasted_iota(jnp.int32, (512, 1), 0)
    q_row = (q_row // 128) * BLOCK + q_row % BLOCK
    eye = lax.broadcasted_iota(jnp.int32, (128, 128), 0) == lax.broadcasted_iota(
        jnp.int32, (128, 128), 1
    )
    for peer in range(4):
        s = lax.dot_general(
            q_refs[peer][:512, :],
            pool_ref[:, :HEAD_SIZE],
            (((1,), (1,)), ((), ())),
            preferred_element_type=jnp.float32,
        )
        s = jnp.where(pool_end <= (z * 4 + owners[peer]) * SPAN + q_row, s * SCALE, NEGATIVE)
        m = jnp.maximum(jnp.max(s, axis=1, keepdims=True), FLOOR)
        p = jnp.exp(s - m)
        total = jnp.sum(p, axis=1, keepdims=True)
        acc = jnp.dot(
            p.astype(jnp.bfloat16), pool_ref[:, HEAD_SIZE:], preferred_element_type=jnp.float32
        )
        some = total > 0.0
        total = jnp.where(some, total, 1.0)
        lse = jnp.where(some, m + jnp.log(total), FLOOR)
        out = (acc / total).astype(jnp.bfloat16)
        for qb in range(4):
            for head in range(2):
                for half in range(2):
                    at = qb * 128 + head * BLOCK + half * 32
                    out_ref[
                        owners[peer] * 2 + half,
                        128 + qb * 32 : 128 + (qb + 1) * 32,
                        head * HEAD_SIZE : (head + 1) * HEAD_SIZE,
                    ] = out[at : at + 32]
            spread = jnp.where(eye, lse[qb * 128 : (qb + 1) * 128], 0.0)
            g = 16 + peer * 4 + qb
            lse_ref[g : g + 1, :] = jnp.sum(spread, axis=0, keepdims=True)

    for first_peer in range(0, 4, PEERS):
        members = [(first_peer + i // 4, i % 4) for i in range(4 * PEERS)]
        for slot in range(4 * PEERS):
            acc_ref[slot] = jnp.zeros((HEAD_SIZE, HEAD_SIZE), jnp.float32)
            m_ref[slot] = jnp.full((1, HEAD_SIZE), FLOOR, jnp.float32)
            l_ref[slot] = jnp.zeros((1, HEAD_SIZE), jnp.float32)

        def group(k, carry, members=members):
            for slot, (peer, qb) in enumerate(members):
                g = peer * 4 + qb
                qpos = (z * 4 + owners[peer]) * SPAN + qb * BLOCK + lane
                keys, values, bases, biases = [], [], [], []
                for e in range(PER_STEP):
                    idx = ids_ref[g, k * PER_STEP + e]
                    none = idx < 0
                    safe = jnp.where(none, 0, idx)
                    first = pl.multiple_of(safe * BLOCK, BLOCK)
                    keys.append(kv_ref[pl.ds(first, BLOCK), :HEAD_SIZE])
                    values.append(kv_ref[pl.ds(first, BLOCK), HEAD_SIZE:])
                    base = ((z - safe // 4) * 4 + y) * SPAN + (safe % 4) * BLOCK
                    bases.append(jnp.where(none, 1 << 30, base))
                    biases.append(bias_ref[g, k * PER_STEP + e])
                kg = jnp.concatenate(keys, 0)
                vg = jnp.concatenate(values, 0)
                s = lax.dot_general(
                    kg,
                    q_refs[peer][qb * 128 : (qb + 1) * 128, :],
                    (((1,), (1,)), ((), ())),
                    preferred_element_type=jnp.float32,
                )
                slabs = []
                for e in range(PER_STEP):
                    slab = s[e * BLOCK : (e + 1) * BLOCK] * SCALE + biases[e]
                    seen = row <= (qpos - bases[e])
                    slabs.append(jnp.where(seen, slab, NEGATIVE))
                s = jnp.concatenate(slabs, 0)
                m_old = m_ref[slot]
                m_new = jnp.maximum(m_old, jnp.max(s, axis=0, keepdims=True))
                alpha = jnp.exp(m_old - m_new)
                p = jnp.exp(s - m_new)
                total = l_ref[slot] * alpha + jnp.sum(p, axis=0, keepdims=True)
                pv = lax.dot_general(
                    vg,
                    p.astype(jnp.bfloat16),
                    (((0,), (0,)), ((), ())),
                    preferred_element_type=jnp.float32,
                )
                acc_ref[slot] = acc_ref[slot] * alpha + pv
                m_ref[slot] = m_new
                l_ref[slot] = total
            return carry

        steps = meta_ref[0, 2 + first_peer]
        for peer in range(first_peer + 1, first_peer + PEERS):
            steps = jnp.maximum(steps, meta_ref[0, 2 + peer])
        lax.fori_loop(0, steps, group, 0)
        for slot, (peer, qb) in enumerate(members):
            total = l_ref[slot]
            some = total > 0.0
            total = jnp.where(some, total, 1.0)
            store(peer, qb, 0, acc_ref[slot] / total)
            g = peer * 4 + qb
            lse_ref[g : g + 1, :] = jnp.where(some, m_ref[slot] + jnp.log(total), FLOOR)

    for peer in range(4):
        rows = []
        for branch in range(2):
            at = branch * 16 + peer * 4
            lse = lse_ref[at : at + 4, :]
            wide = jnp.concatenate(
                [
                    jnp.concatenate([lse[0:1], lse[1:2]], 1),
                    jnp.concatenate([lse[2:3], lse[3:4]], 1),
                ],
                0,
            )
            rows += split_three(wide)
        rows.append(jnp.zeros((STATS - 12, 2 * HEAD_SIZE), jnp.float32))
        block = jnp.concatenate(rows, 0).astype(jnp.bfloat16)
        for half in range(2):
            out_ref[owners[peer] * 2 + half, SPAN : SPAN + STATS, :] = block


def attend(meta, ids, bias, queries, chunks):
    whole = lambda shape: pl.BlockSpec(shape, lambda i, *_: (0,) * len(shape))
    return pl.pallas_call(
        attend_kernel,
        grid_spec=pltpu.PrefetchScalarGridSpec(
            num_scalar_prefetch=3,
            grid=(1,),
            in_specs=[whole((QROWS, HEAD_SIZE))] * 2
            + [whole((2 * QROWS, HEAD_SIZE))]
            + [whole((SPAN + POOLED, 2 * HEAD_SIZE))] * RING,
            out_specs=whole((8, SPAN + STATS, 2 * HEAD_SIZE)),
            scratch_shapes=[
                pltpu.VMEM((RING * SPAN, 2 * HEAD_SIZE), jnp.bfloat16),
                pltpu.VMEM((RING * POOLED, 2 * HEAD_SIZE), jnp.bfloat16),
                pltpu.VMEM((4 * PEERS, HEAD_SIZE, HEAD_SIZE), jnp.float32),
                pltpu.VMEM((4 * PEERS, 1, HEAD_SIZE), jnp.float32),
                pltpu.VMEM((4 * PEERS, 1, HEAD_SIZE), jnp.float32),
                pltpu.VMEM((32, HEAD_SIZE), jnp.float32),
            ],
        ),
        out_shape=jax.ShapeDtypeStruct((8, SPAN + STATS, 2 * HEAD_SIZE), jnp.bfloat16),
        compiler_params=pltpu.CompilerParams(vmem_limit_bytes=20 << 20),
        name="attend",
    )(meta, ids, bias, *queries, *chunks)


def merge_kernel(meta_ref, got_ref, gate_ref, own_ref, other_ref, out_ref, log_ref, t_ref, att_ref):
    c = meta_ref[0]
    for branch in range(2):
        pieces = []
        for core in range(2):
            lses = []
            for peer in range(4):
                block = got_ref[peer * 2 + core, SPAN : SPAN + STATS, :].astype(jnp.float32)
                at = branch * 6
                lses.append(block[at : at + 2] + block[at + 2 : at + 4] + block[at + 4 : at + 6])
            top = jnp.maximum(jnp.maximum(lses[0], lses[1]), jnp.maximum(lses[2], lses[3]))
            parts = [jnp.exp(v - top) for v in lses]
            total = (parts[0] + parts[1]) + (parts[2] + parts[3])
            if branch == 0:
                log_ref[core] = top + jnp.log(total)
            for v in parts:
                share = v / total
                pieces.append(share[:, :HEAD_SIZE])
                pieces.append(share[:, HEAD_SIZE:])
        t_ref[branch] = jnp.transpose(jnp.concatenate(pieces, 0))
    for core in range(2):
        for qb in range(4):
            for head in range(2):
                cols = slice(head * HEAD_SIZE, (head + 1) * HEAD_SIZE)
                total = jnp.zeros((32, HEAD_SIZE), jnp.float32)
                for branch in range(2):
                    share = t_ref[branch, pl.ds(head * BLOCK + c * 32, 32), :]
                    part = jnp.zeros((32, HEAD_SIZE), jnp.float32)
                    for peer in range(4):
                        col = (core * 4 + peer) * 4 + (qb % 2) * 2 + qb // 2
                        first = branch * 128 + qb * 32
                        value = got_ref[peer * 2 + core, first : first + 32, cols]
                        part = part + value.astype(jnp.float32) * share[:, col : col + 1]
                    g = (1 - branch) * 4 + core * 2 + head
                    total = total + part * gate_ref[qb * 32 : (qb + 1) * 32, g : g + 1]
                att_ref[core, qb * 32 : (qb + 1) * 32, cols] = total.astype(jnp.bfloat16)
    shares = jnp.dot(att_ref[c], own_ref[...], preferred_element_type=jnp.float32)
    shares = shares + jnp.dot(att_ref[1 - c], other_ref[...], preferred_element_type=jnp.float32)
    out_ref[...] = shares.astype(jnp.bfloat16)


def merge(meta, got, gates, own_weight, other_weight):
    whole = lambda shape: pl.BlockSpec(shape, lambda i, *_: (0,) * len(shape))
    width = own_weight.shape[1]
    return pl.pallas_call(
        merge_kernel,
        grid_spec=pltpu.PrefetchScalarGridSpec(
            num_scalar_prefetch=1,
            grid=(1,),
            in_specs=[
                whole((8, SPAN + STATS, 2 * HEAD_SIZE)),
                whole((128, 8)),
                whole((2 * HEAD_SIZE, width)),
                whole((2 * HEAD_SIZE, width)),
            ],
            out_specs=[whole((128, width)), whole((2, 2, 2 * HEAD_SIZE))],
            scratch_shapes=[
                pltpu.VMEM((2, HEAD_SIZE, 32), jnp.float32),
                pltpu.VMEM((2, 128, 2 * HEAD_SIZE), jnp.bfloat16),
            ],
        ),
        out_shape=[
            jax.ShapeDtypeStruct((128, width), jnp.bfloat16),
            jax.ShapeDtypeStruct((2, 2, 2 * HEAD_SIZE), jnp.float32),
        ],
        compiler_params=pltpu.CompilerParams(vmem_limit_bytes=12 << 20),
        name="merge",
    )(meta, got, gates, own_weight, other_weight)


def lists_kernel(
    place_ref, own_ref, side_ref, far_ref, last_ref, meta_ref, ids_ref, bias_ref
):
    f32 = jnp.float32
    z = place_ref[2]
    y = place_ref[3]
    kb = lax.broadcasted_iota(jnp.int32, (BLOCK, 128), 0)
    lane = lax.broadcasted_iota(jnp.int32, (BLOCK, 128), 1)
    pick_row = lax.broadcasted_iota(jnp.int32, (128, 128), 0)
    pick_lane = lax.broadcasted_iota(jnp.int32, (128, 128), 1)
    per_list = (pick_row // 32 == pick_lane).astype(f32)
    square = (BLOCK, BLOCK)
    earlier = lax.broadcasted_iota(jnp.int32, square, 1) < lax.broadcasted_iota(
        jnp.int32, square, 0
    )
    meta_lane = lax.broadcasted_iota(jnp.int32, (8, 128), 1)
    meta = jnp.where(meta_lane == 0, z, jnp.where(meta_lane == 1, y, 0))
    for peer, ref in enumerate((own_ref, side_ref, far_ref, last_ref)):
        picks = ref[0:1, :].astype(f32).astype(jnp.int32)
        mine = ((picks >> 2) & 3) == y
        slot = ((z - (picks >> 4)) & (RING - 1)) * 4 + (picks & 3)
        slot = jnp.where(mine, slot, -1)
        counts = jnp.dot((slot == kb).astype(f32), per_list, preferred_element_type=f32)
        present = jnp.where(counts > 0.5, 1.0, 0.0)
        rank = jnp.dot(earlier.astype(f32), present, preferred_element_type=f32)
        rank = jnp.where(counts > 0.5, rank, 1000.0).astype(jnp.int32)
        for qb in range(4):
            hit = rank[:, qb : qb + 1] == lane
            g = peer * 4 + qb
            ids_ref[g : g + 1, :] = (
                jnp.sum(jnp.where(hit, kb + 1, 0), axis=0, keepdims=True) - 1
            )
            times = jnp.sum(
                jnp.where(hit, counts[:, qb : qb + 1], 0.0), axis=0, keepdims=True
            )
            bias_ref[g : g + 1, :] = jnp.log(jnp.maximum(times, 1.0))
        longest = jnp.max(jnp.sum(present, axis=0, keepdims=True)).astype(jnp.int32)
        steps = (longest + PER_STEP - 1) // PER_STEP
        meta = jnp.where(meta_lane == 2 + peer, steps, meta)
    meta_ref[...] = meta


def block_lists(place, own, side, far):
    last = lambda at: pl.BlockSpec((16, 128), lambda i, *_: (at, 0))
    whole = lambda rows: pl.BlockSpec((rows, 128), lambda i, *_: (0, 0))
    return pl.pallas_call(
        lists_kernel,
        grid_spec=pltpu.PrefetchScalarGridSpec(
            num_scalar_prefetch=1,
            grid=(1,),
            in_specs=[last(32), last(32), last(32), last(65)],
            out_specs=[whole(8), whole(16), whole(16)],
        ),
        out_shape=[
            jax.ShapeDtypeStruct((8, 128), jnp.int32),
            jax.ShapeDtypeStruct((16, 128), jnp.int32),
            jax.ShapeDtypeStruct((16, 128), jnp.float32),
        ],
        compiler_params=pltpu.CompilerParams(vmem_limit_bytes=8 << 20),
        name="lists",
    )(place, own, side, far, far)


def shards(
    tokens,
    query_weight,
    key_matrix,
    value_matrix,
    gate_weight,
    key_pool_weight,
    value_pool_weight,
    out_weight,
    chosen,
):
    z, y = lax.axis_index("z"), lax.axis_index("y")
    x, c = lax.axis_index("x"), lax.axis_index("c")
    own = z * 4 + y
    group = x * 2 + c
    f32, bf16 = jnp.float32, jnp.bfloat16

    cosines, sines = rotary_tables(own, np.arange(SPAN))
    place = jnp.stack([own, group, z, y]).astype(jnp.int32)
    chunk = project(place, tokens, key_matrix, value_matrix, key_pool_weight.T, value_pool_weight.T)
    query_proj = jnp.dot(tokens, query_weight, preferred_element_type=f32)
    query_proj = query_proj.reshape(SPAN, 2, HEAD_SIZE)
    queries = rotate(query_proj, cosines[:, None, :], sines[:, None, :]).astype(bf16)
    by_block = queries.reshape(4, BLOCK, 2, HEAD_SIZE).transpose(0, 2, 1, 3)
    picks = jnp.pad(chosen.astype(bf16).reshape(1, 128), ((0, 15), (0, 0)))
    sent = jnp.concatenate([by_block.reshape(512, HEAD_SIZE), picks], 0)

    chunks = [chunk] + [None] * (RING - 1)
    up = down = chunk
    for k in range(1, RING // 2 + 1):
        up = lax.ppermute(up, "z", [(i, i + 1) for i in range(k - 1, RING - 1)])
        chunks[k] = up
        if k < RING // 2:
            moved = [(i - k) % RING for i in range(RING // 2 - 1)]
            down = lax.ppermute(down, "z", [((i + 1) % RING, i) for i in moved])
            chunks[RING - k] = down
        if k == 2:
            side = lax.ppermute(sent, "y", [(i, i ^ 1) for i in range(4)])
        if k == 4:
            both = jnp.concatenate([sent, side], 0)
            far = lax.ppermute(both, "y", [(i, i ^ 2) for i in range(4)])
    other_weight = lax.ppermute(out_weight, "c", [(0, 1), (1, 0)])
    meta, ids, bias = block_lists(place, sent, side, far)

    own_tokens = lax.dynamic_index_in_dim(
        tokens.reshape(4, 2, 32, -1), c, 1, keepdims=False
    ).reshape(128, -1)
    gate_cols = lax.dynamic_slice_in_dim(gate_weight, x * 4, 4, 2)
    gates = jax.nn.sigmoid(
        jnp.einsum("td,bdh->tbh", own_tokens, gate_cols, preferred_element_type=f32)
    ).reshape(128, 8)

    partial = attend(meta, ids, bias, (sent, side, far), chunks)
    got = lax.all_to_all(partial, ("y", "c"), 0, 0, tiled=True)
    shares, log_all = merge(
        c.astype(jnp.int32).reshape(1), got, gates, out_weight, other_weight
    )
    log_own = lax.dynamic_index_in_dim(log_all, c, 0, keepdims=False)
    log_sums = log_own.reshape(4, 2, BLOCK).transpose(0, 2, 1).reshape(SPAN, 2)
    pieces = lax.all_to_all(shares.reshape(4, 32, -1), "x", 0, 0, tiled=True)
    mixed = jnp.sum(pieces.astype(f32), axis=0).astype(bf16)
    return (mixed, log_sums)


def solution(mesh):
    split = Mesh(mesh.devices.reshape(16, 4, 4, 2), ("z", "y", "x", "c"))
    tp = ("x", "c")
    placed = (
        P(KV, None),
        P(None, tp),
        P(None, tp),
        P(None, tp),
        P(),
        P(),
        P(),
        P(tp, None),
        P(KV, None),
    )
    return jax.shard_map(
        shards,
        mesh=split,
        in_specs=placed,
        out_specs=(P(KV + tp, None), P(KV, tp)),
        check_vma=False,
    )
```

```python
import jax
import jax.numpy as jnp
import numpy as np
from jax import lax
from jax.experimental import pallas as pl
from jax.experimental.pallas import tpu as pltpu
from jax.sharding import Mesh
from jax.sharding import PartitionSpec as P


HEAD_SIZE = 128
BLOCK = 64
POOL_STRIDE = 16
THETA = 10000.0
NEGATIVE = -1e30
FLOOR = -1e29
KV = ("z", "y")
SPAN = 256
STATS = 16
PER_STEP = 10
PEERS = 2
POOLED = 16
RING = 16
QROWS = 528
UP_LEAPS = (3,)
DOWN_LEAPS = (3,)
SCALE = HEAD_SIZE**-0.5


def rotary_tables(start, offsets):
    half = HEAD_SIZE // 2
    inverse = THETA ** (-np.arange(half, dtype=np.float64) / half)
    local = np.asarray(offsets, np.float64)[:, None] * inverse[None, :]
    cos_l = jnp.asarray(np.cos(local), jnp.float32)
    sin_l = jnp.asarray(np.sin(local), jnp.float32)
    starts = np.arange(64, dtype=np.float64)[:, None] * SPAN * inverse[None, :]
    cos_s = lax.dynamic_slice_in_dim(jnp.asarray(np.cos(starts), jnp.float32), start, 1, 0)
    sin_s = lax.dynamic_slice_in_dim(jnp.asarray(np.sin(starts), jnp.float32), start, 1, 0)
    return cos_l * cos_s - sin_l * sin_s, sin_l * cos_s + cos_l * sin_s


def rotate(value, cosines, sines):
    half = HEAD_SIZE // 2
    front, back = value[..., :half], value[..., half:]
    return jnp.concatenate([front * cosines - back * sines, back * cosines + front * sines], -1)


def project_kernel(
    meta_ref, tok_ref, wk_ref, wv_ref, kmix_ref, vmix_ref, local_ref, span_ref, out_ref, k_ref, v_ref
):
    step = pl.program_id(0)

    @pl.when(step == 0)
    def _():
        k_ref[...] = jnp.zeros_like(k_ref)
        v_ref[...] = jnp.zeros_like(v_ref)

    both = jnp.concatenate([wk_ref[...], wv_ref[...]], 1)
    kv = jnp.dot(tok_ref[...], both, preferred_element_type=jnp.float32)
    k_ref[...] += kv[:, :HEAD_SIZE]
    v_ref[...] += kv[:, HEAD_SIZE:]

    @pl.when(step == pl.num_programs(0) - 1)
    def _():
        own = meta_ref[0]
        group = meta_ref[1]
        cos_s = span_ref[0, pl.ds(own, 1), :]
        sin_s = span_ref[1, pl.ds(own, 1), :]

        def rotated(value, cos_l, sin_l):
            cosines = cos_l * cos_s - sin_l * sin_s
            sines = sin_l * cos_s + cos_l * sin_s
            sign = lax.broadcasted_iota(jnp.int32, (1, HEAD_SIZE), 1) < HEAD_SIZE // 2
            turned = pltpu.roll(value, HEAD_SIZE // 2, 1)
            return value * cosines + jnp.where(sign, -turned, turned) * sines

        def pooled(value, mix_ref):
            shape = (POOL_STRIDE, POOL_STRIDE)
            eye = lax.broadcasted_iota(jnp.int32, shape, 0) == lax.broadcasted_iota(
                jnp.int32, shape, 1
            )
            mix = jnp.where(eye, mix_ref[pl.ds(group, 1), :], 0.0)
            mix = jnp.sum(mix, axis=1, keepdims=True)
            mixed = value.reshape(POOLED, POOL_STRIDE, HEAD_SIZE) * mix[None]
            return jnp.sum(mixed, axis=1)

        keys = k_ref[...]
        values = v_ref[...]
        out_ref[:SPAN, :HEAD_SIZE] = rotated(
            keys, local_ref[0, :SPAN], local_ref[1, :SPAN]
        ).astype(jnp.bfloat16)
        out_ref[:SPAN, HEAD_SIZE:] = values.astype(jnp.bfloat16)
        out_ref[SPAN:, :HEAD_SIZE] = rotated(
            pooled(keys, kmix_ref), local_ref[0, SPAN:], local_ref[1, SPAN:]
        ).astype(jnp.bfloat16)
        out_ref[SPAN:, HEAD_SIZE:] = pooled(values, vmix_ref).astype(jnp.bfloat16)


def project(meta, tokens, key_matrix, value_matrix, key_mix, value_mix):
    half = HEAD_SIZE // 2
    inverse = THETA ** (-np.arange(half, dtype=np.float64) / half)
    inverse = np.concatenate([inverse, inverse])
    offsets = np.concatenate(
        [np.arange(SPAN), np.arange(POOLED) * POOL_STRIDE + POOL_STRIDE - 1]
    ).astype(np.float64)
    local = offsets[:, None] * inverse[None, :]
    spans = np.arange(64, dtype=np.float64)[:, None] * SPAN * inverse[None, :]
    local = jnp.asarray(np.stack([np.cos(local), np.sin(local)]), jnp.float32)
    spans = jnp.asarray(np.stack([np.cos(spans), np.sin(spans)]), jnp.float32)
    depth = 2048
    return pl.pallas_call(
        project_kernel,
        grid_spec=pltpu.PrefetchScalarGridSpec(
            num_scalar_prefetch=1,
            grid=(tokens.shape[1] // depth,),
            in_specs=[
                pl.BlockSpec((SPAN, depth), lambda i, *_: (0, i)),
                pl.BlockSpec((depth, HEAD_SIZE), lambda i, *_: (i, 0)),
                pl.BlockSpec((depth, HEAD_SIZE), lambda i, *_: (i, 0)),
                pl.BlockSpec((8, POOL_STRIDE), lambda i, *_: (0, 0)),
                pl.BlockSpec((8, POOL_STRIDE), lambda i, *_: (0, 0)),
                pl.BlockSpec((2, SPAN + POOLED, HEAD_SIZE), lambda i, *_: (0, 0, 0)),
                pl.BlockSpec((2, 64, HEAD_SIZE), lambda i, *_: (0, 0, 0)),
            ],
            out_specs=pl.BlockSpec((SPAN + POOLED, 2 * HEAD_SIZE), lambda i, *_: (0, 0)),
            scratch_shapes=[
                pltpu.VMEM((SPAN, HEAD_SIZE), jnp.float32),
                pltpu.VMEM((SPAN, HEAD_SIZE), jnp.float32),
            ],
        ),
        out_shape=jax.ShapeDtypeStruct((SPAN + POOLED, 2 * HEAD_SIZE), jnp.bfloat16),
        name="project",
    )(meta, tokens, key_matrix, value_matrix, key_mix, value_mix, local, spans)


def split_three(value):
    high = value.astype(jnp.bfloat16).astype(jnp.float32)
    rest = value - high
    middle = rest.astype(jnp.bfloat16).astype(jnp.float32)
    return [high, middle, rest - middle]


def attend_kernel(meta_ref, ids_ref, bias_ref, *refs):
    own_ref, side_ref, far_ref = refs[:3]
    chunk_refs = refs[3 : 3 + RING]
    out_ref, kv_ref, pool_ref, acc_ref, m_ref, l_ref, lse_ref = refs[3 + RING :]
    z = meta_ref[0, 0]
    y = meta_ref[0, 1]
    q_refs = [own_ref, side_ref, far_ref.at[:QROWS], far_ref.at[QROWS:]]
    owners = [y ^ peer for peer in range(4)]
    for o in range(RING):
        kv_ref[o * SPAN : (o + 1) * SPAN, :] = chunk_refs[o][:SPAN, :]
        pool_ref[o * POOLED : (o + 1) * POOLED, :] = chunk_refs[o][SPAN:, :]
    row = lax.broadcasted_iota(jnp.int32, (BLOCK, HEAD_SIZE), 0)
    lane = lax.broadcasted_iota(jnp.int32, (1, HEAD_SIZE), 1)
    lane = jnp.where(lane >= BLOCK, lane - BLOCK, lane)

    def store(peer, qb, first, normal):
        out = jnp.transpose(normal).astype(jnp.bfloat16)
        for half in range(2):
            for head in range(2):
                at = head * BLOCK + half * 32
                out_ref[
                    owners[peer] * 2 + half,
                    first + qb * 32 : first + (qb + 1) * 32,
                    head * HEAD_SIZE : (head + 1) * HEAD_SIZE,
                ] = out[at : at + 32]

    col = lax.broadcasted_iota(jnp.int32, (1, RING * POOLED), 1)
    offset = col // POOLED
    pool_at = ((z - offset) * 4 + y) * POOLED + col % POOLED
    pool_end = pool_at * POOL_STRIDE + POOL_STRIDE - 1
    pool_end = jnp.where(offset > z, 1 << 30, jnp.where(pool_at == 0, 0, pool_end))
    q_row = lax.broadcasted_iota(jnp.int32, (512, 1), 0)
    q_row = (q_row // 128) * BLOCK + q_row % BLOCK
    eye = lax.broadcasted_iota(jnp.int32, (128, 128), 0) == lax.broadcasted_iota(
        jnp.int32, (128, 128), 1
    )
    for peer in range(4):
        s = lax.dot_general(
            q_refs[peer][:512, :],
            pool_ref[:, :HEAD_SIZE],
            (((1,), (1,)), ((), ())),
            preferred_element_type=jnp.float32,
        )
        s = jnp.where(pool_end <= (z * 4 + owners[peer]) * SPAN + q_row, s * SCALE, NEGATIVE)
        m = jnp.maximum(jnp.max(s, axis=1, keepdims=True), FLOOR)
        p = jnp.exp(s - m)
        total = jnp.sum(p, axis=1, keepdims=True)
        acc = jnp.dot(
            p.astype(jnp.bfloat16), pool_ref[:, HEAD_SIZE:], preferred_element_type=jnp.float32
        )
        some = total > 0.0
        total = jnp.where(some, total, 1.0)
        lse = jnp.where(some, m + jnp.log(total), FLOOR)
        out = (acc / total).astype(jnp.bfloat16)
        for qb in range(4):
            for head in range(2):
                for half in range(2):
                    at = qb * 128 + head * BLOCK + half * 32
                    out_ref[
                        owners[peer] * 2 + half,
                        128 + qb * 32 : 128 + (qb + 1) * 32,
                        head * HEAD_SIZE : (head + 1) * HEAD_SIZE,
                    ] = out[at : at + 32]
            spread = jnp.where(eye, lse[qb * 128 : (qb + 1) * 128], 0.0)
            g = 16 + peer * 4 + qb
            lse_ref[g : g + 1, :] = jnp.sum(spread, axis=0, keepdims=True)

    for first_peer in range(0, 4, PEERS):
        members = [(first_peer + i // 4, i % 4) for i in range(4 * PEERS)]
        for slot in range(4 * PEERS):
            acc_ref[slot] = jnp.zeros((HEAD_SIZE, HEAD_SIZE), jnp.float32)
            m_ref[slot] = jnp.full((1, HEAD_SIZE), FLOOR, jnp.float32)
            l_ref[slot] = jnp.zeros((1, HEAD_SIZE), jnp.float32)

        def group(k, carry, members=members):
            for slot, (peer, qb) in enumerate(members):
                g = peer * 4 + qb
                qpos = (z * 4 + owners[peer]) * SPAN + qb * BLOCK + lane
                keys, values, bases, biases = [], [], [], []
                for e in range(PER_STEP):
                    idx = ids_ref[g, k * PER_STEP + e]
                    none = idx < 0
                    safe = jnp.where(none, 0, idx)
                    first = pl.multiple_of(safe * BLOCK, BLOCK)
                    keys.append(kv_ref[pl.ds(first, BLOCK), :HEAD_SIZE])
                    values.append(kv_ref[pl.ds(first, BLOCK), HEAD_SIZE:])
                    base = ((z - safe // 4) * 4 + y) * SPAN + (safe % 4) * BLOCK
                    bases.append(jnp.where(none, 1 << 30, base))
                    biases.append(bias_ref[g, k * PER_STEP + e])
                kg = jnp.concatenate(keys, 0)
                vg = jnp.concatenate(values, 0)
                s = lax.dot_general(
                    kg,
                    q_refs[peer][qb * 128 : (qb + 1) * 128, :],
                    (((1,), (1,)), ((), ())),
                    preferred_element_type=jnp.float32,
                )
                slabs = []
                for e in range(PER_STEP):
                    slab = s[e * BLOCK : (e + 1) * BLOCK] * SCALE + biases[e]
                    seen = row <= (qpos - bases[e])
                    slabs.append(jnp.where(seen, slab, NEGATIVE))
                s = jnp.concatenate(slabs, 0)
                m_old = m_ref[slot]
                m_new = jnp.maximum(m_old, jnp.max(s, axis=0, keepdims=True))
                alpha = jnp.exp(m_old - m_new)
                p = jnp.exp(s - m_new)
                total = l_ref[slot] * alpha + jnp.sum(p, axis=0, keepdims=True)
                pv = lax.dot_general(
                    vg,
                    p.astype(jnp.bfloat16),
                    (((0,), (0,)), ((), ())),
                    preferred_element_type=jnp.float32,
                )
                acc_ref[slot] = acc_ref[slot] * alpha + pv
                m_ref[slot] = m_new
                l_ref[slot] = total
            return carry

        steps = meta_ref[0, 2 + first_peer]
        for peer in range(first_peer + 1, first_peer + PEERS):
            steps = jnp.maximum(steps, meta_ref[0, 2 + peer])
        lax.fori_loop(0, steps, group, 0)
        for slot, (peer, qb) in enumerate(members):
            total = l_ref[slot]
            some = total > 0.0
            total = jnp.where(some, total, 1.0)
            store(peer, qb, 0, acc_ref[slot] / total)
            g = peer * 4 + qb
            lse_ref[g : g + 1, :] = jnp.where(some, m_ref[slot] + jnp.log(total), FLOOR)

    for peer in range(4):
        rows = []
        for branch in range(2):
            at = branch * 16 + peer * 4
            lse = lse_ref[at : at + 4, :]
            wide = jnp.concatenate(
                [
                    jnp.concatenate([lse[0:1], lse[1:2]], 1),
                    jnp.concatenate([lse[2:3], lse[3:4]], 1),
                ],
                0,
            )
            rows += split_three(wide)
        rows.append(jnp.zeros((STATS - 12, 2 * HEAD_SIZE), jnp.float32))
        block = jnp.concatenate(rows, 0).astype(jnp.bfloat16)
        for half in range(2):
            out_ref[owners[peer] * 2 + half, SPAN : SPAN + STATS, :] = block


def attend(meta, ids, bias, queries, chunks):
    whole = lambda shape: pl.BlockSpec(shape, lambda i, *_: (0,) * len(shape))
    return pl.pallas_call(
        attend_kernel,
        grid_spec=pltpu.PrefetchScalarGridSpec(
            num_scalar_prefetch=3,
            grid=(1,),
            in_specs=[whole((QROWS, HEAD_SIZE))] * 2
            + [whole((2 * QROWS, HEAD_SIZE))]
            + [whole((SPAN + POOLED, 2 * HEAD_SIZE))] * RING,
            out_specs=whole((8, SPAN + STATS, 2 * HEAD_SIZE)),
            scratch_shapes=[
                pltpu.VMEM((RING * SPAN, 2 * HEAD_SIZE), jnp.bfloat16),
                pltpu.VMEM((RING * POOLED, 2 * HEAD_SIZE), jnp.bfloat16),
                pltpu.VMEM((4 * PEERS, HEAD_SIZE, HEAD_SIZE), jnp.float32),
                pltpu.VMEM((4 * PEERS, 1, HEAD_SIZE), jnp.float32),
                pltpu.VMEM((4 * PEERS, 1, HEAD_SIZE), jnp.float32),
                pltpu.VMEM((32, HEAD_SIZE), jnp.float32),
            ],
        ),
        out_shape=jax.ShapeDtypeStruct((8, SPAN + STATS, 2 * HEAD_SIZE), jnp.bfloat16),
        compiler_params=pltpu.CompilerParams(vmem_limit_bytes=20 << 20),
        name="attend",
    )(meta, ids, bias, *queries, *chunks)


def merge_kernel(meta_ref, got_ref, gate_ref, own_ref, other_ref, out_ref, log_ref, t_ref, att_ref):
    c = meta_ref[0]
    for branch in range(2):
        pieces = []
        for core in range(2):
            lses = []
            for peer in range(4):
                block = got_ref[peer * 2 + core, SPAN : SPAN + STATS, :].astype(jnp.float32)
                at = branch * 6
                lses.append(block[at : at + 2] + block[at + 2 : at + 4] + block[at + 4 : at + 6])
            top = jnp.maximum(jnp.maximum(lses[0], lses[1]), jnp.maximum(lses[2], lses[3]))
            parts = [jnp.exp(v - top) for v in lses]
            total = (parts[0] + parts[1]) + (parts[2] + parts[3])
            if branch == 0:
                log_ref[core] = top + jnp.log(total)
            for v in parts:
                share = v / total
                pieces.append(share[:, :HEAD_SIZE])
                pieces.append(share[:, HEAD_SIZE:])
        t_ref[branch] = jnp.transpose(jnp.concatenate(pieces, 0))
    for core in range(2):
        for qb in range(4):
            for head in range(2):
                cols = slice(head * HEAD_SIZE, (head + 1) * HEAD_SIZE)
                total = jnp.zeros((32, HEAD_SIZE), jnp.float32)
                for branch in range(2):
                    share = t_ref[branch, pl.ds(head * BLOCK + c * 32, 32), :]
                    part = jnp.zeros((32, HEAD_SIZE), jnp.float32)
                    for peer in range(4):
                        col = (core * 4 + peer) * 4 + (qb % 2) * 2 + qb // 2
                        first = branch * 128 + qb * 32
                        value = got_ref[peer * 2 + core, first : first + 32, cols]
                        part = part + value.astype(jnp.float32) * share[:, col : col + 1]
                    g = (1 - branch) * 4 + core * 2 + head
                    total = total + part * gate_ref[qb * 32 : (qb + 1) * 32, g : g + 1]
                att_ref[core, qb * 32 : (qb + 1) * 32, cols] = total.astype(jnp.bfloat16)
    shares = jnp.dot(att_ref[c], own_ref[...], preferred_element_type=jnp.float32)
    shares = shares + jnp.dot(att_ref[1 - c], other_ref[...], preferred_element_type=jnp.float32)
    out_ref[...] = shares.astype(jnp.bfloat16)


def merge(meta, got, gates, own_weight, other_weight):
    whole = lambda shape: pl.BlockSpec(shape, lambda i, *_: (0,) * len(shape))
    width = own_weight.shape[1]
    return pl.pallas_call(
        merge_kernel,
        grid_spec=pltpu.PrefetchScalarGridSpec(
            num_scalar_prefetch=1,
            grid=(1,),
            in_specs=[
                whole((8, SPAN + STATS, 2 * HEAD_SIZE)),
                whole((128, 8)),
                whole((2 * HEAD_SIZE, width)),
                whole((2 * HEAD_SIZE, width)),
            ],
            out_specs=[whole((128, width)), whole((2, 2, 2 * HEAD_SIZE))],
            scratch_shapes=[
                pltpu.VMEM((2, HEAD_SIZE, 32), jnp.float32),
                pltpu.VMEM((2, 128, 2 * HEAD_SIZE), jnp.bfloat16),
            ],
        ),
        out_shape=[
            jax.ShapeDtypeStruct((128, width), jnp.bfloat16),
            jax.ShapeDtypeStruct((2, 2, 2 * HEAD_SIZE), jnp.float32),
        ],
        compiler_params=pltpu.CompilerParams(vmem_limit_bytes=12 << 20),
        name="merge",
    )(meta, got, gates, own_weight, other_weight)


def lists_kernel(
    place_ref, own_ref, side_ref, far_ref, last_ref, meta_ref, ids_ref, bias_ref
):
    f32 = jnp.float32
    z = place_ref[2]
    y = place_ref[3]
    kb = lax.broadcasted_iota(jnp.int32, (BLOCK, 128), 0)
    lane = lax.broadcasted_iota(jnp.int32, (BLOCK, 128), 1)
    pick_row = lax.broadcasted_iota(jnp.int32, (128, 128), 0)
    pick_lane = lax.broadcasted_iota(jnp.int32, (128, 128), 1)
    per_list = (pick_row // 32 == pick_lane).astype(f32)
    square = (BLOCK, BLOCK)
    earlier = lax.broadcasted_iota(jnp.int32, square, 1) < lax.broadcasted_iota(
        jnp.int32, square, 0
    )
    meta_lane = lax.broadcasted_iota(jnp.int32, (8, 128), 1)
    meta = jnp.where(meta_lane == 0, z, jnp.where(meta_lane == 1, y, 0))
    for peer, ref in enumerate((own_ref, side_ref, far_ref, last_ref)):
        picks = ref[0:1, :].astype(f32).astype(jnp.int32)
        mine = ((picks >> 2) & 3) == y
        slot = ((z - (picks >> 4)) & (RING - 1)) * 4 + (picks & 3)
        slot = jnp.where(mine, slot, -1)
        counts = jnp.dot((slot == kb).astype(f32), per_list, preferred_element_type=f32)
        present = jnp.where(counts > 0.5, 1.0, 0.0)
        rank = jnp.dot(earlier.astype(f32), present, preferred_element_type=f32)
        rank = jnp.where(counts > 0.5, rank, 1000.0).astype(jnp.int32)
        for qb in range(4):
            hit = rank[:, qb : qb + 1] == lane
            g = peer * 4 + qb
            ids_ref[g : g + 1, :] = (
                jnp.sum(jnp.where(hit, kb + 1, 0), axis=0, keepdims=True) - 1
            )
            times = jnp.sum(
                jnp.where(hit, counts[:, qb : qb + 1], 0.0), axis=0, keepdims=True
            )
            bias_ref[g : g + 1, :] = jnp.log(jnp.maximum(times, 1.0))
        longest = jnp.max(jnp.sum(present, axis=0, keepdims=True)).astype(jnp.int32)
        steps = (longest + PER_STEP - 1) // PER_STEP
        meta = jnp.where(meta_lane == 2 + peer, steps, meta)
    meta_ref[...] = meta


def block_lists(place, own, side, far):
    last = lambda at: pl.BlockSpec((16, 128), lambda i, *_: (at, 0))
    whole = lambda rows: pl.BlockSpec((rows, 128), lambda i, *_: (0, 0))
    return pl.pallas_call(
        lists_kernel,
        grid_spec=pltpu.PrefetchScalarGridSpec(
            num_scalar_prefetch=1,
            grid=(1,),
            in_specs=[last(32), last(32), last(32), last(65)],
            out_specs=[whole(8), whole(16), whole(16)],
        ),
        out_shape=[
            jax.ShapeDtypeStruct((8, 128), jnp.int32),
            jax.ShapeDtypeStruct((16, 128), jnp.int32),
            jax.ShapeDtypeStruct((16, 128), jnp.float32),
        ],
        compiler_params=pltpu.CompilerParams(vmem_limit_bytes=8 << 20),
        name="lists",
    )(place, own, side, far, far)


def shards(
    tokens,
    query_weight,
    key_matrix,
    value_matrix,
    gate_weight,
    key_pool_weight,
    value_pool_weight,
    out_weight,
    chosen,
):
    z, y = lax.axis_index("z"), lax.axis_index("y")
    x, c = lax.axis_index("x"), lax.axis_index("c")
    own = z * 4 + y
    group = x * 2 + c
    f32, bf16 = jnp.float32, jnp.bfloat16

    cosines, sines = rotary_tables(own, np.arange(SPAN))
    place = jnp.stack([own, group, z, y]).astype(jnp.int32)
    chunk = project(place, tokens, key_matrix, value_matrix, key_pool_weight.T, value_pool_weight.T)
    query_proj = jnp.dot(tokens, query_weight, preferred_element_type=f32)
    query_proj = query_proj.reshape(SPAN, 2, HEAD_SIZE)
    queries = rotate(query_proj, cosines[:, None, :], sines[:, None, :]).astype(bf16)
    by_block = queries.reshape(4, BLOCK, 2, HEAD_SIZE).transpose(0, 2, 1, 3)
    picks = jnp.pad(chosen.astype(bf16).reshape(1, 128), ((0, 15), (0, 0)))
    sent = jnp.concatenate([by_block.reshape(512, HEAD_SIZE), picks], 0)

    chunks = [chunk] + [None] * (RING - 1)

    def step_up(k):
        leap = k if k in UP_LEAPS else 1
        pairs = [(i, i + leap) for i in range(k - leap, RING - leap)]
        source = chunk if k == leap else chunks[k - 1]
        chunks[k] = lax.ppermute(source, "z", pairs)

    def step_down(k):
        leap = k if k in DOWN_LEAPS else 1
        ends = [(i - k) % RING for i in range(RING // 2 - 1)]
        pairs = [((i + leap) % RING, i) for i in ends]
        source = chunk if k == leap else chunks[RING - k + 1]
        chunks[RING - k] = lax.ppermute(source, "z", pairs)

    for k in range(1, RING // 2 + 1):
        step_up(k)
        if k < RING // 2:
            step_down(k)
    side = lax.ppermute(sent, "y", [(i, i ^ 1) for i in range(4)])
    both = jnp.concatenate([sent, side], 0)
    far = lax.ppermute(both, "y", [(i, i ^ 2) for i in range(4)])
    other_weight = lax.ppermute(out_weight, "c", [(0, 1), (1, 0)])
    meta, ids, bias = block_lists(place, sent, side, far)

    own_tokens = lax.dynamic_index_in_dim(
        tokens.reshape(4, 2, 32, -1), c, 1, keepdims=False
    ).reshape(128, -1)
    gate_cols = lax.dynamic_slice_in_dim(gate_weight, x * 4, 4, 2)
    gates = jax.nn.sigmoid(
        jnp.einsum("td,bdh->tbh", own_tokens, gate_cols, preferred_element_type=f32)
    ).reshape(128, 8)

    partial = attend(meta, ids, bias, (sent, side, far), chunks)
    got = lax.all_to_all(partial, ("y", "c"), 0, 0, tiled=True)
    shares, log_all = merge(
        c.astype(jnp.int32).reshape(1), got, gates, out_weight, other_weight
    )
    log_own = lax.dynamic_index_in_dim(log_all, c, 0, keepdims=False)
    log_sums = log_own.reshape(4, 2, BLOCK).transpose(0, 2, 1).reshape(SPAN, 2)
    pieces = lax.all_to_all(shares.reshape(4, 32, -1), "x", 0, 0, tiled=True)
    mixed = jnp.sum(pieces.astype(f32), axis=0).astype(bf16)
    return (mixed, log_sums)


def solution(mesh):
    split = Mesh(mesh.devices.reshape(16, 4, 4, 2), ("z", "y", "x", "c"))
    tp = ("x", "c")
    placed = (
        P(KV, None),
        P(None, tp),
        P(None, tp),
        P(None, tp),
        P(),
        P(),
        P(),
        P(tp, None),
        P(KV, None),
    )
    return jax.shard_map(
        shards,
        mesh=split,
        in_specs=placed,
        out_specs=(P(KV + tp, None), P(KV, tp)),
        check_vma=False,
    )
```
